128 devices in a mesh: ep: 128 (over z, y, x, core).
Axes of the slice: x: 4, y: 4, z: 4, core: 2. Of those that a mesh axis runs over, the one named last changes fastest.
Arguments:
- tokens: bfloat16 [1024, 2048], P('ep'), may hold values from -6 to 6
- cache_keys: bfloat16 [1024, 1024, 128], P('ep'), may hold values from -80 to 80
- cache_values: bfloat16 [1024, 1024, 128], P('ep'), may hold values from -6 to 6
- cum_gates: float32 [1024, 1024, 2], P('ep'), may hold values from -1024 to 0, as said below
- lengths: int32 [1024], P('ep'), may hold values from 128 to 1024
- query_weight: bfloat16 [2048, 2048], replicated, may hold values from -0.125 to 0.125
- key_weight: bfloat16 [2048, 128], replicated, may hold values from -0.125 to 0.125
- value_weight: bfloat16 [2048, 128], replicated, may hold values from -0.125 to 0.125
- forget_weight: bfloat16 [2048, 2], replicated, may hold values from -0.125 to 0.125
- out_weight: bfloat16 [2048, 2048], P('ep'), may hold values from -1 to 1
- norm_gain: float32 [2, 2048], replicated, may hold values from 0.1 to 1.9
- norm_bias: float32 [2, 2048], replicated, may hold values from -1 to 1
- dense_gate_weight: bfloat16 [2048, 5632], P(None, 'ep'), may hold values from -0.125 to 0.125
- dense_up_weight: bfloat16 [2048, 5632], P(None, 'ep'), may hold values from -0.125 to 0.125
- dense_down_weight: bfloat16 [5632, 2048], P('ep'), may hold values from -0.078125 to 0.078125
- dense_scale: float32 [2048], replicated, may hold values from 0.2 to 1.5
- expert_gate_weight: bfloat16 [2048, 57344], P(None, 'ep'), may hold values from -0.125 to 0.125
- expert_up_weight: bfloat16 [2048, 57344], P(None, 'ep'), may hold values from -0.125 to 0.125
- expert_down_weight: bfloat16 [57344, 2048], P('ep'), may hold values from -0.0625 to 0.0625
- routes: int32 [1024, 2], replicated, may hold values from 0 to 7, all different within a row; in each aligned block of 8 rows (0 to 7, 8 to 15, ...) at most 3 rows name the same one
- route_weights: float32 [1024, 2], replicated, may hold values from 0.2 to 1
Outputs:
- output: bfloat16 [1024, 2048], P('ep')
The draws below stay inside these ranges and needn't reach their ends.
Inputs may be any that keep to these rules, and one draw needn't show every extreme that they name: `routes`: each row names 2 different experts; the rows of one device (8 aligned rows) name one expert at most 3 times. `cum_gates`: non-increasing along positions.
All inputs are finite; a program needn't handle non-finite values.
Results may differ from the reference program's by a relative error of at most 0.012.
Values may be sent and summed in bfloat16 or wider, within the bound.
A program may use at most 128 MiB of HBM per device.

```python
import math
import jax
import jax.numpy as jnp
import numpy as np
from jax import lax

D = 2048
HEADS = 32
HEAD_DIM = 64
KEY_VALUE_HEADS = 2
FF_DENSE = 5632
FF_EXPERT = 7168
EXPERTS = 8
TOP = 2
SEQ_DEV = 8
CACHE_SLOTS = 1024
SEQUENCE_COUNT = 1024
CAP = 3
N_EP = 128


def draw_cache_keys(key, part):
    key_rows = jax.random.split(key, 1)
    shape = (SEQUENCE_COUNT, CACHE_SLOTS, KEY_VALUE_HEADS * HEAD_DIM)
    return jax.random.normal(key_rows[0], shape, jnp.float32).astype(jnp.bfloat16)


def draw_cum_gates(key, part):
    key_rows = jax.random.split(key, 7)
    devices = SEQUENCE_COUNT // SEQ_DEV
    share_fast = 0.5
    fast = jax.random.uniform(key_rows[0], (SEQUENCE_COUNT, 1, KEY_VALUE_HEADS)) < share_fast
    fast_rate = jnp.exp(jax.random.uniform(key_rows[1], (SEQUENCE_COUNT, 1, KEY_VALUE_HEADS), jnp.float32, math.log(1.0 / 100.0), math.log(1.0 / 30.0)))
    slow_rate = jnp.exp(jax.random.uniform(key_rows[2], (SEQUENCE_COUNT, 1, KEY_VALUE_HEADS), jnp.float32, math.log(0.1), math.log(0.4))) / CACHE_SLOTS
    decay_rate = jnp.where(fast, fast_rate, slow_rate)
    per_device_ratio = jnp.exp(jax.random.uniform(key_rows[3], (devices, 1, 1), jnp.float32, 0.0, math.log(3.0)))
    per_device_ratio = jnp.repeat(per_device_ratio, SEQ_DEV, axis=0)
    coarse_estimate = jnp.exp(jax.random.uniform(key_rows[4], (SEQUENCE_COUNT, CACHE_SLOTS, KEY_VALUE_HEADS), jnp.float32, math.log(0.5), math.log(2.0)))
    spike_position = jax.random.randint(key_rows[5], (SEQUENCE_COUNT, 1, KEY_VALUE_HEADS, 2), 0, CACHE_SLOTS)
    decay_penalty = jax.random.uniform(key_rows[6], (SEQUENCE_COUNT, 1, KEY_VALUE_HEADS, 2), jnp.float32, 0.2, 0.5)
    current_slot = jnp.arange(CACHE_SLOTS, dtype=jnp.int32)[None, :, None, None]
    spike_amount = jnp.sum(jnp.where(current_slot == spike_position, -jnp.log(1.0 - decay_penalty), 0.0), axis=3)
    step_total = decay_rate * per_device_ratio * coarse_estimate + spike_amount
    return jnp.cumsum(-step_total, axis=1).astype(jnp.float32)


def with_ends(result, key, least, largest):
    longest = result.shape.index(max(result.shape))
    spots = []
    for shift in (0, 1):
        where = [jax.random.randint(jax.random.fold_in(key, axis), (), 0, length) for axis, length in enumerate(result.shape)]
        where[longest] = (where[longest] + shift) % result.shape[longest]
        spots.append(tuple(where))
    return result.at[spots[0]].set(least).at[spots[1]].set(largest)


def levels(stream_key, dims, cuts, smallest, top_value):
    level, own = 1.0, jax.random.fold_in(stream_key, 6)
    for dim, parts in cuts:
        heights = jnp.exp(jax.random.uniform(jax.random.fold_in(own, dim), (parts,), jnp.float32, smallest / len(cuts), top_value / len(cuts)))
        level = level * jnp.repeat(heights, dims[dim] // parts).reshape([-1 if axis == dim else 1 for axis in range(len(dims))])
    return level


def routed_block(stream_key, own, number, rows, count, top, reach, slope):
    ranking = jax.random.permutation(stream_key, count)
    crowded, common = load_shares(count, rows * top, reach, slope, True), load_shares(count, rows * top, reach, slope, False)
    places = jnp.arange(count)

    def named(tallies, turn):
        used = int((tallies > 0).sum())
        fixed = max(1, used // 4)
        shifted = fixed + (places - fixed + turn * (used - fixed)) % max(1, count - fixed)
        return jnp.zeros((count,), jnp.int32).at[ranking[jnp.where(places < fixed, places, shifted)]].set(jnp.asarray(tallies, jnp.int32))

    tallies = jnp.where(number % 4 == 0, named(crowded, number // 4), named(common, number - number // 4 - 1))
    mixed = jax.random.permutation(jax.random.fold_in(own, 3), count)
    source_of, taker = mixed[0:count // 2 * 2:2], mixed[1:count // 2 * 2:2]
    slack = jnp.minimum(tallies[source_of] - 1, reach - tallies[taker]) // 2
    slack = jnp.where((source_of == ranking[0]) | (taker == ranking[0]) | (tallies[taker] == 0), 0, jnp.maximum(slack, 0))
    shifted = jax.random.randint(jax.random.fold_in(own, 4), (count // 2,), 0, 1 << 20) % (slack + 1)
    tallies = tallies.at[source_of].add(-shifted).at[taker].add(shifted)
    items = jnp.searchsorted(jnp.cumsum(tallies), jnp.arange(rows * top), side="right").astype(jnp.int32)
    table = items.reshape(top, rows).T
    table = table[jax.random.permutation(jax.random.fold_in(own, 1), rows)]
    turn = jax.random.randint(jax.random.fold_in(own, 2), (rows, 1), 0, top)
    return jnp.take_along_axis(table, (jnp.arange(top)[None, :] + turn) % top, axis=1)


def load_shares(count, total, bound, skew, full):
    weights = [(1 << 20) // math.isqrt(rank ** skew) + 1 for rank in range(1, count + 1)]
    largest = bound if full else min(bound, max(-(-total // count), total * weights[0] // sum(weights)))
    least = 1 if total - largest >= count - 1 else 0
    holding, spare = [largest] + [least] * (count - 1), total - largest - least * (count - 1)
    while spare > 0:
        movable = [i for i in range(1, count) if holding[i] < largest] or [i for i in range(1, count) if holding[i] < bound]
        whole, remaining = sum([weights[i] for i in movable]), spare
        for i in movable:
            more = min(bound - holding[i], max(1, remaining * weights[i] // whole), spare)
            holding[i] = holding[i] + more
            spare = spare - more
    return np.array(holding)


def normal_values(stream_key, shape, scale, reach, cuts=(), held_as=jnp.bfloat16):
    level = levels(stream_key, shape, cuts, -0.22, 0.18) if cuts else 1.0
    values = jax.random.normal(stream_key, shape, jnp.float32) * scale * level
    return jnp.minimum(jnp.maximum(values, -reach), reach).astype(held_as)


def setup_inputs(seed: int = 0) -> dict:
    keys = jax.random.split(jax.random.key(seed), 22)
    tokens = normal_values(keys[0], (SEQUENCE_COUNT, D), 1.0, 6.0, ((0, 128),))
    cache_keys = draw_cache_keys(jax.random.fold_in(keys[21], 71), 0)
    cache_values = normal_values(keys[2], (SEQUENCE_COUNT, CACHE_SLOTS, KEY_VALUE_HEADS * HEAD_DIM), 1.0, 6.0, ((0, 128),))
    cum_gates = draw_cum_gates(jax.random.fold_in(keys[21], 71), 0)
    lengths = with_ends(jax.random.randint(keys[4], (SEQUENCE_COUNT,), CACHE_SLOTS // 8, CACHE_SLOTS + 1), jax.random.fold_in(keys[4], 1), CACHE_SLOTS // 8, CACHE_SLOTS).astype(jnp.int32)
    query_weight = normal_values(keys[5], (D, HEADS * HEAD_DIM), D ** -0.5, 0.125)
    key_weight = normal_values(keys[6], (D, KEY_VALUE_HEADS * HEAD_DIM), D ** -0.5, 0.125)
    value_weight = normal_values(keys[7], (D, KEY_VALUE_HEADS * HEAD_DIM), D ** -0.5, 0.125)
    forget_weight = normal_values(keys[8], (D, KEY_VALUE_HEADS), D ** -0.5, 0.125)
    out_weight = normal_values(keys[9], (HEADS * HEAD_DIM, D), (HEADS * HEAD_DIM // 64) ** -0.5, 1.0, ((0, 128),))
    norm_gain = jnp.clip(1.0 + 0.18 * jax.random.normal(keys[10], (2, D), jnp.float32), 0.1, 1.9)
    norm_bias = normal_values(keys[11], (2, D), 0.2, 1.0, (), jnp.float32)
    dense_gate_weight = normal_values(keys[12], (D, FF_DENSE), D ** -0.5, 0.125, ((1, 128),))
    dense_up_weight = normal_values(keys[13], (D, FF_DENSE), D ** -0.5, 0.125, ((1, 128),))
    dense_down_weight = normal_values(keys[14], (FF_DENSE, D), FF_DENSE ** -0.5, 0.078125, ((0, 128),))
    dense_scale = jnp.clip(jax.random.uniform(keys[15], (D,), jnp.float32, 0.2, 1.5), 0.2, 1.5)
    expert_gate_weight = normal_values(keys[16], (D, EXPERTS * FF_EXPERT), D ** -0.5, 0.125, ((1, 128),))
    expert_up_weight = normal_values(keys[17], (D, EXPERTS * FF_EXPERT), D ** -0.5, 0.125, ((1, 128),))
    expert_down_weight = normal_values(keys[18], (EXPERTS * FF_EXPERT, D), FF_EXPERT ** -0.5, 0.0625, ((0, 128),))
    routes_keys = jax.random.split(jax.random.fold_in(keys[19], 1), SEQUENCE_COUNT // SEQ_DEV)
    routes_turns = jax.random.permutation(jax.random.fold_in(keys[19], 3), SEQUENCE_COUNT // SEQ_DEV)
    routes = jax.vmap(lambda own, number: routed_block(jax.random.fold_in(keys[19], 2), own, number, SEQ_DEV, EXPERTS, TOP, CAP, 2))(routes_keys, routes_turns).reshape((SEQUENCE_COUNT, TOP))
    route_weights = jnp.clip(jax.random.uniform(keys[20], (SEQUENCE_COUNT, TOP), jnp.float32, 0.2, 1.0), 0.2, 1.0)
    return dict(tokens=tokens, cache_keys=cache_keys, cache_values=cache_values, cum_gates=cum_gates, lengths=lengths, query_weight=query_weight, key_weight=key_weight, value_weight=value_weight, forget_weight=forget_weight, out_weight=out_weight, norm_gain=norm_gain, norm_bias=norm_bias, dense_gate_weight=dense_gate_weight, dense_up_weight=dense_up_weight, dense_down_weight=dense_down_weight, dense_scale=dense_scale, expert_gate_weight=expert_gate_weight, expert_up_weight=expert_up_weight, expert_down_weight=expert_down_weight, routes=routes, route_weights=route_weights)


residual_scale = 1.4142135
norm_eps = 1e-05

def layer_norm(values, gain_row, shift_row):
    centre = lax.optimization_barrier(jnp.mean(values, axis=-1, keepdims=True))
    centred = values - centre
    spread = lax.optimization_barrier(jnp.mean(centred * centred, axis=-1, keepdims=True))
    return (centred * lax.rsqrt(spread + norm_eps) * gain_row + shift_row).astype(jnp.bfloat16)

def attend_block(inputs):
    queries, cached_keys, cached_values, gate_sums, length_row, fresh_key, fresh_value, fresh_gate = inputs
    amount = queries.shape[0]
    grouped = HEADS // KEY_VALUE_HEADS
    query_grid_four = queries.astype(jnp.float32).reshape(amount, KEY_VALUE_HEADS, grouped, HEAD_DIM)
    key_four = cached_keys.astype(jnp.float32).reshape(amount, CACHE_SLOTS, KEY_VALUE_HEADS, HEAD_DIM)
    value_four = cached_values.astype(jnp.float32).reshape(amount, CACHE_SLOTS, KEY_VALUE_HEADS, HEAD_DIM)
    self_key_row = fresh_key.astype(jnp.float32).reshape(amount, KEY_VALUE_HEADS, HEAD_DIM)
    own_value = fresh_value.astype(jnp.float32).reshape(amount, KEY_VALUE_HEADS, HEAD_DIM)
    ratio_value = HEAD_DIM ** (-0.5)
    latest = jnp.take_along_axis(gate_sums, (length_row - 1).astype(jnp.int32)[:, None, None], axis=1)
    offsets = jnp.transpose(latest - gate_sums + fresh_gate[:, None, :], (0, 2, 1))
    past = jnp.einsum('bkgd,blkd->bkgl', query_grid_four, key_four) * ratio_value + offsets[:, :, None, :]
    live = jnp.arange(CACHE_SLOTS, dtype=jnp.int32)[None, :] < length_row[:, None]
    past = jnp.where(live[:, None, None, :], past, -jnp.inf)
    self_part = jnp.einsum('rifs,ris->rif', query_grid_four, self_key_row) * ratio_value
    highest = jnp.maximum(lax.optimization_barrier(jnp.max(past, axis=-1)), self_part)
    past_exp = jnp.exp(past - highest[..., None])
    own_exp = jnp.exp(self_part - highest)
    denominator = lax.optimization_barrier(jnp.sum(past_exp, axis=-1)) + own_exp
    past_weight = lax.optimization_barrier((past_exp / denominator[..., None]).astype(jnp.bfloat16)).astype(jnp.float32)
    own_weight = lax.optimization_barrier((own_exp / denominator).astype(jnp.bfloat16)).astype(jnp.float32)
    mixed = jnp.einsum('bkgl,blkd->bkgd', past_weight, value_four) + own_weight[..., None] * own_value[:, :, None, :]
    return mixed.reshape(amount, HEADS * HEAD_DIM).astype(jnp.bfloat16)

def expert_mix(settled, expert_gate, expert_up, expert_down, routes, route_weights):
    shards = N_EP // EXPERTS
    part_width = FF_EXPERT // shards
    chosen = routes.reshape(N_EP, SEQ_DEV, TOP)
    shares = route_weights.reshape(N_EP, SEQ_DEV, TOP)
    expert_ids = jnp.arange(EXPERTS, dtype=jnp.int32)
    picked = (chosen[..., None] == expert_ids).astype(jnp.int32)
    hits = lax.optimization_barrier(jnp.sum(picked, axis=2))
    portion = lax.optimization_barrier(jnp.sum(picked.astype(jnp.float32) * shares[..., None], axis=2))
    ranks = jnp.cumsum(hits, axis=1) - hits
    slot_ids = jnp.arange(CAP, dtype=jnp.int32)
    matched = (hits[..., None] * (ranks[..., None] == slot_ids).astype(jnp.int32)).astype(jnp.float32)
    by_source = settled.astype(jnp.float32).reshape(N_EP, SEQ_DEV, D)

    def one_expert(running, expert):
        select = lax.dynamic_index_in_dim(matched, expert, 2, keepdims=False)
        weight_here = lax.dynamic_index_in_dim(portion, expert, 2, keepdims=False)
        slot_rows = jnp.einsum('nsc,nsd->ncd', select, by_source, precision=lax.Precision.HIGHEST)
        slot_rows = slot_rows.reshape(N_EP * CAP, D).astype(jnp.bfloat16)
        gate_cols = lax.dynamic_slice_in_dim(expert_gate, expert * FF_EXPERT, FF_EXPERT, 1)
        up_cols = lax.dynamic_slice_in_dim(expert_up, expert * FF_EXPERT, FF_EXPERT, 1)
        down_rows = lax.dynamic_slice_in_dim(expert_down, expert * FF_EXPERT, FF_EXPERT, 0)
        gate_val = jnp.dot(slot_rows, gate_cols, preferred_element_type=jnp.float32)
        up_val = jnp.dot(slot_rows, up_cols, preferred_element_type=jnp.float32)
        hidden = (jax.nn.silu(gate_val) * up_val).astype(jnp.bfloat16)
        pieces = jnp.einsum('rgf,gfd->rgd', hidden.astype(jnp.float32).reshape(N_EP * CAP, shards, part_width), down_rows.astype(jnp.float32).reshape(shards, part_width, D))
        pieces = lax.optimization_barrier(pieces.astype(jnp.bfloat16)).astype(jnp.float32)
        summed = lax.optimization_barrier(jnp.sum(pieces, axis=1)).reshape(N_EP, CAP, D)
        placed = jnp.einsum('nsc,ncd->nsd', select, summed, precision=lax.Precision.HIGHEST)
        return (running + weight_here[..., None] * placed, None)
    combined, unused = lax.scan(one_expert, jnp.zeros((N_EP, SEQ_DEV, D), jnp.float32), jnp.arange(EXPERTS, dtype=jnp.int32))
    return combined.reshape(N_EP * SEQ_DEV, D)

def reference(tokens, cache_keys, cache_values, cum_gates, lengths, query_weight, key_weight, value_weight, forget_weight, out_weight, norm_gain, norm_bias, dense_gate_weight, dense_up_weight, dense_down_weight, dense_scale, expert_gate_weight, expert_up_weight, expert_down_weight, routes, route_weights):
    query = jnp.dot(tokens, query_weight, preferred_element_type=jnp.float32).astype(jnp.bfloat16)
    new_key = jnp.dot(tokens, key_weight, preferred_element_type=jnp.float32).astype(jnp.bfloat16)
    new_value = jnp.dot(tokens, value_weight, preferred_element_type=jnp.float32).astype(jnp.bfloat16)
    new_gate = jax.nn.log_sigmoid(jnp.dot(tokens, forget_weight, preferred_element_type=jnp.float32))

    def blocks(array):
        return array.reshape((N_EP, SEQ_DEV) + array.shape[1:])
    attended = lax.map(attend_block, (blocks(query), blocks(cache_keys), blocks(cache_values), blocks(cum_gates), blocks(lengths), blocks(new_key), blocks(new_value), blocks(new_gate)))
    attended = attended.reshape(SEQUENCE_COUNT, HEADS * HEAD_DIM)
    projected = jnp.dot(attended, out_weight, preferred_element_type=jnp.float32)
    settled = layer_norm(residual_scale * tokens.astype(jnp.float32) + projected, norm_gain[0], norm_bias[0])
    dense_gate = jnp.dot(settled, dense_gate_weight, preferred_element_type=jnp.float32)
    dense_up = jnp.dot(settled, dense_up_weight, preferred_element_type=jnp.float32)
    dense_hidden = (jax.nn.silu(dense_gate) * dense_up).astype(jnp.bfloat16)
    dense_out = jnp.dot(dense_hidden, dense_down_weight, preferred_element_type=jnp.float32)
    expert_out = expert_mix(settled, expert_gate_weight, expert_up_weight, expert_down_weight, routes, route_weights)
    ffn = expert_out + dense_scale * dense_out
    return layer_norm(residual_scale * settled.astype(jnp.float32) + ffn, norm_gain[1], norm_bias[1])
```

```python
import functools

import jax
import jax.numpy as jnp
from jax import lax
from jax.experimental import pallas as pl
from jax.experimental.pallas import tpu as pltpu
from jax.sharding import PartitionSpec as P

N = 128
D = 2048
SEQ = 8
SLOTS = 1024
HID = 448
DEN = 44
HPAD = 512
residual_scale = 1.4142135
norm_eps = 1e-05
MESH = pl.DeviceIdType.MESH
NT = (((1,), (1,)), ((), ()))
F32 = jnp.float32
BF16 = jnp.bfloat16

COLOURS = ((0, 768, (2, 1, 0)), (768, 640, (0, 2, 1)), (1408, 640, (1, 0, 2)))


def layer_norm(values, gain_row, shift_row):
    centre = jnp.mean(values, axis=-1, keepdims=True)
    centred = values - centre
    spread = jnp.mean(centred * centred, axis=-1, keepdims=True)
    return (centred * lax.rsqrt(spread + norm_eps) * gain_row + shift_row).astype(BF16)


def remote(src, dst, send, recv, peer):
    return pltpu.make_async_remote_copy(
        src_ref=src, dst_ref=dst, send_sem=send, recv_sem=recv, device_id=(peer,), device_id_type=MESH
    )


def wait_bytes(ref, sem):
    pltpu.make_async_copy(ref, ref, sem).wait()


def attention_kernel(
    len_ref, tok_h, wq_h, wk_h, wv_h, fw_h, kc_h, vc_h, cg_h, ow_h, gain_h, bias_h,
    out_ref,
    tok, wq, wk, wv, fw, kc, vc, cg, ow, gain, bias,
    q3, o3, nk, nv, ng, wbuf, abuf, psend, prec,
    lsem, wsend, wrecv, asend, arecv, fsend, psem, rsem,
):
    me = lax.axis_index("ep")
    group = me // 16
    slot = lax.rem(me, 16)
    core = lax.rem(me, 2)
    partner = me + 1 - 2 * core
    barrier = pltpu.get_barrier_semaphore()

    def hello(i, carry):
        pl.semaphore_signal(barrier, inc=1, device_id=(lax.rem(me + i, N),), device_id_type=MESH)
        return carry

    lax.fori_loop(1, N, hello, 0)

    loads = {}

    def load(name, src, dst):
        loads[name] = pltpu.make_async_copy(src, dst, lsem.at[len(loads)])
        loads[name].start()

    load("tok", tok_h, tok)
    load("ow", ow_h, ow)
    for k in range(8):
        load(("wq", k), wq_h.at[pl.ds(k * 256, 256)], wq.at[pl.ds(k * 256, 256)])
    load("wk", wk_h, wk)
    load("wv", wv_h, wv)
    load("fw", fw_h, fw)
    load("cg", cg_h, cg)
    load("kc", kc_h, kc)
    load("vc", vc_h, vc)
    load("gain", gain_h, gain)
    load("bias", bias_h, bias)
    loads["tok"].wait()

    acc = jnp.zeros((SEQ, D), F32)
    for k in range(8):
        loads[("wq", k)].wait()
        acc = acc + jnp.dot(
            tok[:, k * 256:(k + 1) * 256], wq[k * 256:(k + 1) * 256, :], preferred_element_type=F32
        )
    acc = acc.astype(BF16).astype(F32)
    loads["wk"].wait()
    loads["wv"].wait()
    loads["fw"].wait()
    nk[...] = jnp.dot(tok[...], wk[...], preferred_element_type=F32).astype(BF16).astype(F32)
    nv[...] = jnp.dot(tok[...], wv[...], preferred_element_type=F32).astype(BF16).astype(F32)
    tok32 = tok[...].astype(F32)
    fw32 = fw[...].astype(F32)
    for j in range(2):
        x = jnp.sum(tok32 * fw32[j:j + 1, :], axis=-1, keepdims=True)
        gate = jnp.minimum(x, 0.0) - jnp.log1p(jnp.exp(-jnp.abs(x)))
        ng[j] = jnp.broadcast_to(gate, (SEQ, 128))

    lane = lax.broadcasted_iota(jnp.int32, (SEQ, 128), 1)
    for h in range(32):
        j = h // 16
        tile = acc[:, (h // 2) * 128:(h // 2 + 1) * 128]
        if h % 2 != j:
            tile = pltpu.roll(tile, 64, 1)
        keep = (lane < 64) if j == 0 else (lane >= 64)
        q3[h * 8:(h + 1) * 8, :] = jnp.where(keep, tile, 0.0)

    loads["ow"].wait()
    own_w = pltpu.make_async_copy(ow.at[:, pl.ds(pl.multiple_of(slot * 128, 128), 128)], wbuf.at[me], psem)
    own_w.start()
    pl.semaphore_wait(barrier, N - 1)
    loads["cg"].wait()
    loads["kc"].wait()
    loads["vc"].wait()
    pos = lax.broadcasted_iota(jnp.int32, (1, SLOTS), 1)

    def sequence(b, carry):
        def push(i, inner):
            off = b * 16 + i + 1

            @pl.when(off < N)
            def _():
                peer = lax.rem(me + off, N)
                column = pl.multiple_of(lax.rem(peer, 16) * 128, 128)
                remote(ow.at[:, pl.ds(column, 128)], wbuf.at[me], wsend, wrecv, peer).start()

            return inner

        lax.fori_loop(0, 16, push, 0)
        used = len_ref[b]
        qb = q3[pl.ds(b, 32, stride=8), :]
        s = lax.dot_general(qb.astype(BF16), kc[b], NT, preferred_element_type=F32)
        own = jnp.sum(qb * nk[pl.ds(b, 1), :], axis=-1, keepdims=True) * 0.125
        halves = []
        for j in range(2):
            sums = cg[b, j:j + 1, :]
            latest = jnp.sum(jnp.where(pos == used - 1, sums, 0.0), axis=-1, keepdims=True)
            offsets = latest - sums + ng[j, pl.ds(b, 1), :][:, 0:1]
            part = s[j * 16:(j + 1) * 16, :] * 0.125 + offsets
            halves.append(jnp.where(pos < used, part, -jnp.inf))
        s = jnp.concatenate(halves, axis=0)
        top = jnp.maximum(jnp.max(s, axis=-1, keepdims=True), own)
        e = jnp.exp(s - top)
        eo = jnp.exp(own - top)
        inv = 1.0 / (jnp.sum(e, axis=-1, keepdims=True) + eo)
        mixed = jnp.dot((e * inv).astype(BF16), vc[b], preferred_element_type=F32)
        mixed = mixed + (eo * inv).astype(BF16).astype(F32) * nv[pl.ds(b, 1), :]
        o3[pl.ds(b, 32, stride=8), :] = mixed
        return carry

    lax.fori_loop(0, SEQ, sequence, 0)
    for t in range(16):
        low = o3[(2 * t) * 8:(2 * t + 1) * 8, :]
        high = o3[(2 * t + 1) * 8:(2 * t + 2) * 8, :]
        if t < 8:
            high = pltpu.roll(high, 64, 1)
        else:
            low = pltpu.roll(low, 64, 1)
        abuf[slot, :, t * 128:(t + 1) * 128] = jnp.where(lane < 64, low, high).astype(BF16)

    sends = []
    for k in range(1, 8):
        other = lax.rem(slot + 2 * k, 16)
        copy = remote(abuf.at[slot], abuf.at[slot], asend.at[k], arecv.at[k], group * 16 + other)
        copy.start()
        sends.append(copy)
    copy = remote(abuf.at[slot], abuf.at[slot], fsend.at[0], arecv.at[8], partner)
    copy.start()
    sends.append(copy)
    for k in range(1, 8):
        source = lax.rem(slot + 16 - 2 * k, 16)
        wait_bytes(abuf.at[source], arecv.at[k])
        copy = remote(abuf.at[source], abuf.at[source], fsend.at[k], arecv.at[8 + k], partner)
        copy.start()
        sends.append(copy)
    for k in range(8):
        wait_bytes(abuf.at[slot], arecv.at[8 + k])
    own_w.wait()
    wait_bytes(wbuf.at[pl.ds(0, N - 1)], wrecv)

    product = jnp.dot(
        abuf[...].reshape(16 * SEQ, D), wbuf[...].reshape(D, 128), preferred_element_type=F32
    )
    psend[...] = product.reshape(16, SEQ, 128)
    for k in range(1, 16):
        other = lax.rem(slot + k, 16)
        remote(psend.at[other], prec.at[slot], rsem.at[0], rsem.at[1], group * 16 + other).start()
    prec[slot] = psend[slot]
    loads["gain"].wait()
    loads["bias"].wait()
    wait_bytes(prec.at[pl.ds(0, 15)], rsem.at[1])
    projected = jnp.concatenate([prec[k] for k in range(16)], axis=-1)
    out_ref[...] = layer_norm(residual_scale * tok32 + projected, gain[0:1, :], bias[0:1, :])
    for copy in sends:
        copy.wait_send()
    wait_bytes(psend.at[pl.ds(0, 15)], rsem.at[0])
    wait_bytes(wbuf.at[pl.ds(0, N - 1)], wsend)


def attention(tokens, keys, values, gates, lengths, qw, kw, vw, fw, ow, gain, bias):
    any_spec = pl.BlockSpec(memory_space=pl.ANY)
    return pl.pallas_call(
        attention_kernel,
        name="attention",
        out_shape=jax.ShapeDtypeStruct((SEQ, D), BF16),
        in_specs=[pl.BlockSpec(memory_space=pltpu.SMEM)] + [any_spec] * 11,
        out_specs=pl.BlockSpec(memory_space=pltpu.VMEM),
        scratch_shapes=[
            pltpu.VMEM((SEQ, D), BF16),
            pltpu.VMEM((D, D), BF16),
            pltpu.VMEM((D, 128), BF16),
            pltpu.VMEM((D, 128), BF16),
            pltpu.VMEM((2, D), BF16),
            pltpu.VMEM((SEQ, SLOTS, 128), BF16),
            pltpu.VMEM((SEQ, SLOTS, 128), BF16),
            pltpu.VMEM((SEQ, 2, SLOTS), F32),
            pltpu.VMEM((16, D), BF16),
            pltpu.VMEM((2, D), F32),
            pltpu.VMEM((2, D), F32),
            pltpu.VMEM((256, 128), F32),
            pltpu.VMEM((256, 128), F32),
            pltpu.VMEM((SEQ, 128), F32),
            pltpu.VMEM((SEQ, 128), F32),
            pltpu.VMEM((2, SEQ, 128), F32),
            pltpu.VMEM((N, 16, 128), BF16),
            pltpu.VMEM((16, SEQ, D), BF16),
            pltpu.VMEM((16, SEQ, 128), F32),
            pltpu.VMEM((16, SEQ, 128), F32),
            pltpu.SemaphoreType.DMA((18,)),
            pltpu.SemaphoreType.DMA,
            pltpu.SemaphoreType.DMA,
            pltpu.SemaphoreType.DMA((8,)),
            pltpu.SemaphoreType.DMA((16,)),
            pltpu.SemaphoreType.DMA((8,)),
            pltpu.SemaphoreType.DMA,
            pltpu.SemaphoreType.DMA((2,)),
        ],
        compiler_params=pltpu.CompilerParams(
            collective_id=0, has_side_effects=True, vmem_limit_bytes=60 * 1024 * 1024
        ),
    )(lengths, tokens, qw, kw, vw, fw, keys, values, gates, ow, gain, bias)


def ffn_kernel(
    settled, eg_h, eu_h, ed_h, dg_h, du_h, dd_h, scale, gain, bias, routes, shares,
    out_ref,
    full, wg, wu, wd, dg, du, dd, hid, portion, part, crec, chip, r1, t1, r2, t2, r3,
    lsem, gsend, grecv, fsend, frecv, csend, crecv, ssend, srecv,
):
    me = lax.axis_index("ep")
    core = lax.rem(me, 2)
    partner = me + 1 - 2 * core
    place = (me // 32, lax.rem(me // 8, 4), lax.rem(me // 2, 4))
    stride = (32, 8, 2)

    def peer_at(axis, d):
        return me + (lax.rem(place[axis] + d, 4) - place[axis]) * stride[axis]

    barrier = pltpu.get_barrier_semaphore()
    peers = [partner] + [peer_at(axis, d) for axis in range(3) for d in (1, 2, 3)]
    for peer in peers:
        pl.semaphore_signal(barrier, inc=1, device_id=(peer,), device_id_type=MESH)

    loads = [
        pltpu.make_async_copy(src, dst, lsem.at[i])
        for i, (src, dst) in enumerate(
            [
                (eg_h, wg.at[pl.ds(0, HID)]),
                (eu_h, wu.at[pl.ds(0, HID)]),
                (ed_h, wd.at[pl.ds(0, HID)]),
                (dg_h, dg),
                (du_h, du),
                (dd_h, dd),
            ]
        )
    ]
    for copy in loads:
        copy.start()
    full[place[0], place[1], place[2], core] = settled[...]
    pl.semaphore_wait(barrier, len(peers))

    def slab(ref, fixed, colour, middle=()):
        start, width, _ = COLOURS[colour]
        index = [slice(None)] * 3
        for axis, value in fixed.items():
            index[axis] = value
        return ref.at[(*index, *middle, slice(None), pl.ds(start, width))]

    sends = []

    def gather_phase(colour, phase):
        order = COLOURS[colour][2]
        axis = order[phase]
        fixed = {a: place[a] for a in order[phase:]}
        for d in (1, 2, 3):
            view = slab(full, fixed, colour, (core,))
            copy = remote(
                view, view, gsend.at[colour, phase, d - 1], grecv.at[colour, phase, d - 1], peer_at(axis, d)
            )
            copy.start()
            sends.append(copy)

    def gather_wait(colour, phase, d):
        order = COLOURS[colour][2]
        axis = order[phase]
        fixed = {a: place[a] for a in order[phase:]}
        fixed[axis] = lax.rem(place[axis] + 4 - d, 4)
        view = slab(full, fixed, colour, (core,))
        wait_bytes(view, grecv.at[colour, phase, d - 1])
        return fixed

    def forward(colour, fixed, number):
        view = slab(full, fixed, colour, (core,))
        copy = remote(view, view, fsend.at[colour, number], frecv.at[colour, number], partner)
        copy.start()
        sends.append(copy)

    for colour in range(3):
        gather_phase(colour, 0)

    expert = me // 16
    share_row = jnp.sum(jnp.where(routes[...] == expert, shares[...], 0.0), axis=0, keepdims=True)
    for i in range(8):
        square = jnp.broadcast_to(share_row[:, i * 128:(i + 1) * 128], (128, 128))
        portion[i * 128:(i + 1) * 128, :] = square.T

    for colour in range(3):
        for d in (1, 2, 3):
            gather_wait(colour, 0, d)
        gather_phase(colour, 1)
    for copy in loads:
        copy.wait()
    for ref, extra in ((wg, dg), (wu, du)):
        ref[480:HPAD, :] = jnp.zeros((HPAD - 480, D), BF16)
        ref[HID:HID + DEN, :] = extra[...]
    wd[480:HPAD, :] = jnp.zeros((HPAD - 480, D), BF16)
    wd[HID:HID + DEN, :] = (dd[...].astype(F32) * scale[...]).astype(BF16)
    for colour in range(3):
        for d in (1, 2, 3):
            gather_wait(colour, 1, d)
        gather_phase(colour, 2)
        last = COLOURS[colour][2][2]
        forward(colour, {last: place[last]}, 0)
    for d in (1, 3, 2):
        for colour in range(3):
            forward(colour, gather_wait(colour, 2, d), d)
    for colour in range(3):
        last = COLOURS[colour][2][2]
        for d in range(4):
            view = slab(full, {last: 0}, colour, (0,))
            wait_bytes(view, frecv.at[colour, d])

    column = lax.broadcasted_iota(jnp.int32, (256, HPAD), 1)

    def hidden(z, carry):
        rows = full[z].reshape(256, D)
        gate = lax.dot_general(rows, wg[...], NT, preferred_element_type=F32)
        up = lax.dot_general(rows, wu[...], NT, preferred_element_type=F32)
        weight = portion[pl.ds(pl.multiple_of(z * 256, 256), 256), :]
        weight = jnp.concatenate([weight] * 4, axis=1)
        value = gate / (1.0 + jnp.exp(-gate)) * up
        value = jnp.where(column < HID, value * weight, value)
        hid[pl.ds(pl.multiple_of(z * 256, 256), 256), :] = value.astype(BF16)
        return carry

    lax.fori_loop(0, 4, hidden, 0)

    def scatter_phase(colour, phase):
        order = COLOURS[colour][2]
        axis = order[2 - phase]
        source = (chip, t1, t2)[phase]
        target = (r1, r2, r3)[phase]
        for d in (1, 2, 3):
            view = slab(source, {a: lax.rem(place[a] + d, 4) if a == axis else 0 if phase and a in order[3 - phase:] else slice(None) for a in range(3)}, colour)
            land = slab(target.at[d - 1], {a: 0 if a in order[2 - phase:] else slice(None) for a in range(3)}, colour)
            copy = remote(
                view, land, ssend.at[colour, phase, d - 1], srecv.at[colour, phase, d - 1], peer_at(axis, d)
            )
            copy.start()
            sends.append(copy)

    return_values = []

    def scatter_sum(colour, phase):
        order = COLOURS[colour][2]
        axis = order[2 - phase]
        source = (chip, t1, t2)[phase]
        target = (r1, r2, r3)[phase]
        own = slab(source, {a: place[a] if a == axis else 0 if phase and a in order[3 - phase:] else slice(None) for a in range(3)}, colour)
        total = own[...].astype(F32)
        for d in (1, 3, 2):
            land = slab(target.at[d - 1], {a: 0 if a in order[2 - phase:] else slice(None) for a in range(3)}, colour)
            wait_bytes(land, srecv.at[colour, phase, d - 1])
            total = total + land[...].astype(F32)
        if phase < 2:
            keep = slab((t1, t2)[phase], {a: 0 if a in order[2 - phase:] else slice(None) for a in range(3)}, colour)
            keep[...] = total.astype(BF16)
        return total

    for colour in range(3):
        start, width, _ = COLOURS[colour]

        def down(z, carry, start=start, width=width):
            block = hid[pl.ds(pl.multiple_of(z * 256, 256), 256), :]
            value = jnp.dot(block, wd[:, start:start + width], preferred_element_type=F32)
            part[z, :, :, :, :, start:start + width] = value.astype(BF16).reshape(4, 4, 2, SEQ, width)
            return carry

        lax.fori_loop(0, 4, down, 0)
        copies = []
        view = part.at[:, :, :, 1 - core, :, pl.ds(start, width)]
        land = crec.at[:, :, :, :, pl.ds(start, width)]
        copy = remote(view, land, csend.at[colour], crecv.at[colour], partner)
        copy.start()
        sends.append(copy)
        copy.wait_recv()

        def join(z, carry, start=start, width=width):
            value = part[z, :, :, core, :, start:start + width].astype(F32)
            value = value + crec[z, :, :, :, start:start + width].astype(F32)
            chip[z, :, :, :, start:start + width] = value.astype(BF16)
            return carry

        lax.fori_loop(0, 4, join, 0)
        scatter_phase(colour, 0)
    for phase in (0, 1):
        for colour in range(3):
            scatter_sum(colour, phase)
            scatter_phase(colour, phase + 1)
    pieces = [scatter_sum(colour, 2) for colour in range(3)]
    ffn = jnp.concatenate(pieces, axis=-1)
    base = residual_scale * settled[...].astype(F32)
    out_ref[...] = layer_norm(base + ffn, gain[1:2, :], bias[1:2, :])
    for copy in sends:
        copy.wait_send()


def ffn(settled, eg, eu, ed, dg, du, dd, scale, gain, bias, routes, shares):
    any_spec = pl.BlockSpec(memory_space=pl.ANY)
    vmem = pl.BlockSpec(memory_space=pltpu.VMEM)
    return pl.pallas_call(
        ffn_kernel,
        name="ffn",
        out_shape=jax.ShapeDtypeStruct((SEQ, D), BF16),
        in_specs=[vmem] + [any_spec] * 6 + [vmem] * 5,
        out_specs=vmem,
        scratch_shapes=[
            pltpu.VMEM((4, 4, 4, 2, SEQ, D), BF16),
            pltpu.VMEM((HPAD, D), BF16),
            pltpu.VMEM((HPAD, D), BF16),
            pltpu.VMEM((HPAD, D), BF16),
            pltpu.VMEM((DEN, D), BF16),
            pltpu.VMEM((DEN, D), BF16),
            pltpu.VMEM((DEN, D), BF16),
            pltpu.VMEM((N * SEQ, HPAD), BF16),
            pltpu.VMEM((N * SEQ, 128), F32),
            pltpu.VMEM((4, 4, 4, 2, SEQ, D), BF16),
            pltpu.VMEM((4, 4, 4, SEQ, D), BF16),
            pltpu.VMEM((4, 4, 4, SEQ, D), BF16),
            pltpu.VMEM((3, 4, 4, 4, SEQ, D), BF16),
            pltpu.VMEM((4, 4, 4, SEQ, D), BF16),
            pltpu.VMEM((3, 4, 4, 4, SEQ, D), BF16),
            pltpu.VMEM((4, 4, 4, SEQ, D), BF16),
            pltpu.VMEM((3, 4, 4, 4, SEQ, D), BF16),
            pltpu.SemaphoreType.DMA((6,)),
            pltpu.SemaphoreType.DMA((3, 3, 3)),
            pltpu.SemaphoreType.DMA((3, 3, 3)),
            pltpu.SemaphoreType.DMA((3, 4)),
            pltpu.SemaphoreType.DMA((3, 4)),
            pltpu.SemaphoreType.DMA((3,)),
            pltpu.SemaphoreType.DMA((3,)),
            pltpu.SemaphoreType.DMA((3, 3, 3)),
            pltpu.SemaphoreType.DMA((3, 3, 3)),
        ],
        compiler_params=pltpu.CompilerParams(
            collective_id=1, has_side_effects=True, vmem_limit_bytes=60 * 1024 * 1024
        ),
    )(settled, eg, eu, ed, dg, du, dd, scale, gain, bias, routes, shares)


def local(
    tokens, cache_keys, cache_values, cum_gates, lengths, query_weight, key_weight, value_weight,
    forget_weight, out_weight, norm_gain, norm_bias, dense_gate_weight, dense_up_weight,
    dense_down_weight, dense_scale, expert_gate_weight, expert_up_weight, expert_down_weight,
    routes, route_weights,
):
    settled = attention(
        tokens, cache_keys, cache_values, jnp.transpose(cum_gates, (0, 2, 1)), lengths, query_weight,
        key_weight, value_weight, forget_weight.T, out_weight, norm_gain, norm_bias,
    )
    return ffn(
        settled, expert_gate_weight.T, expert_up_weight.T, expert_down_weight, dense_gate_weight.T,
        dense_up_weight.T, dense_down_weight, dense_scale.reshape(1, D), norm_gain, norm_bias,
        routes.T, route_weights.T,
    )


def solution(mesh):
    return jax.shard_map(
        local,
        mesh=mesh,
        in_specs=(
            P("ep", None), P("ep", None, None), P("ep", None, None), P("ep", None, None), P("ep"),
            P(), P(), P(), P(), P("ep", None), P(), P(), P(None, "ep"), P(None, "ep"), P("ep", None),
            P(), P(None, "ep"), P(None, "ep"), P("ep", None), P(), P(),
        ),
        out_specs=P("ep", None),
        check_vma=False,
    )
```

```python
import functools

import jax
import jax.numpy as jnp
from jax import lax
from jax.experimental import pallas as pl
from jax.experimental.pallas import tpu as pltpu
from jax.sharding import PartitionSpec as P

N = 128
D = 2048
SEQ = 8
SLOTS = 1024
HID = 448
DEN = 44
HPAD = 512
residual_scale = 1.4142135
norm_eps = 1e-05
MESH = pl.DeviceIdType.MESH
NT = (((1,), (1,)), ((), ()))
F32 = jnp.float32
BF16 = jnp.bfloat16

COLOURS = ((0, 768, (2, 1, 0)), (768, 640, (0, 2, 1)), (1408, 640, (1, 0, 2)))


def layer_norm(values, gain_row, shift_row):
    centre = jnp.mean(values, axis=-1, keepdims=True)
    centred = values - centre
    spread = jnp.mean(centred * centred, axis=-1, keepdims=True)
    return (centred * lax.rsqrt(spread + norm_eps) * gain_row + shift_row).astype(BF16)


def remote(src, dst, send, recv, peer):
    return pltpu.make_async_remote_copy(
        src_ref=src, dst_ref=dst, send_sem=send, recv_sem=recv, device_id=(peer,), device_id_type=MESH
    )


def wait_bytes(ref, sem):
    pltpu.make_async_copy(ref, ref, sem).wait()


def step_kernel(
    len_ref, tok_h, wq_h, wk_h, wv_h, fw_h, kc_h, vc_h, cg_h, ow_h, gain_h, bias_h,
    eg_h, eu_h, ed_h, dg_h, du_h, dd_h, scale_h, routes_h, shares_h,
    out_ref,
    tok, wq, wk, wv, fw, kc, vc, cg, ow, gain, bias,
    q3, o3, nk, nv, ng, wbuf, abuf, psend, prec,
    full, wgu, wd, dg, du, dd, scale, routes, shares, portion, acc, hid,
    part, crec, chip, r1, t1, r2, t2, r3,
    lsem, esem, wsend, wrecv, asend, arecv, fwsend, psem, rsem,
    gsend, grecv, fsend, frecv, csend, crecv, s1send, s1recv, s2send, s2recv, s3send, s3recv,
):
    me = lax.axis_index("ep")
    group = me // 16
    slot = lax.rem(me, 16)
    core = lax.rem(me, 2)
    partner = me + 1 - 2 * core
    place = (me // 32, lax.rem(me // 8, 4), lax.rem(me // 2, 4))
    stride = (32, 8, 2)

    def peer_at(axis, d):
        return me + (lax.rem(place[axis] + d, 4) - place[axis]) * stride[axis]

    loads = {}

    def load(name, src, dst):
        loads[name] = pltpu.make_async_copy(src, dst, lsem.at[len(loads)])
        loads[name].start()

    load("tok", tok_h, tok)
    for k in range(8):
        load(("wq", k), wq_h.at[pl.ds(k * 256, 256)], wq.at[pl.ds(k * 256, 256)])
    load("ow", ow_h, ow)
    load("wk", wk_h, wk)
    load("wv", wv_h, wv)
    load("fw", fw_h, fw)
    load("cg", cg_h, cg)
    load("kc", kc_h, kc)
    load("vc", vc_h, vc)

    barrier = pltpu.get_barrier_semaphore()

    def hello(i, carry):
        pl.semaphore_signal(barrier, inc=1, device_id=(lax.rem(me + i, N),), device_id_type=MESH)
        return carry

    lax.fori_loop(1, N, hello, 0)
    later = []
    for src, dst in (
        (gain_h, gain), (bias_h, bias), (eg_h, wgu.at[pl.ds(0, HID)]), (eu_h, wgu.at[pl.ds(HPAD, HID)]),
        (ed_h, wd.at[pl.ds(0, HID)]), (dg_h, dg), (du_h, du), (dd_h, dd), (scale_h, scale),
        (routes_h, routes), (shares_h, shares),
    ):
        copy = pltpu.make_async_copy(src, dst, esem.at[len(later)])
        copy.start()
        later.append(copy)
    loads["tok"].wait()

    q = jnp.zeros((SEQ, D), F32)
    for k in range(8):
        loads[("wq", k)].wait()
        q = q + jnp.dot(
            tok[:, k * 256:(k + 1) * 256], wq[k * 256:(k + 1) * 256, :], preferred_element_type=F32
        )
    q = q.astype(BF16).astype(F32)
    loads["wk"].wait()
    loads["wv"].wait()
    loads["fw"].wait()
    nk[...] = jnp.dot(tok[...], wk[...], preferred_element_type=F32).astype(BF16).astype(F32)
    nv[...] = jnp.dot(tok[...], wv[...], preferred_element_type=F32).astype(BF16).astype(F32)
    tok32 = tok[...].astype(F32)
    fw32 = fw[...].astype(F32)
    for j in range(2):
        x = jnp.sum(tok32 * fw32[j:j + 1, :], axis=-1, keepdims=True)
        gate = jnp.minimum(x, 0.0) - jnp.log1p(jnp.exp(-jnp.abs(x)))
        ng[j] = jnp.broadcast_to(gate, (SEQ, 128))

    lane = lax.broadcasted_iota(jnp.int32, (SEQ, 128), 1)
    for h in range(32):
        j = h // 16
        tile = q[:, (h // 2) * 128:(h // 2 + 1) * 128]
        if h % 2 != j:
            tile = pltpu.roll(tile, 64, 1)
        keep = (lane < 64) if j == 0 else (lane >= 64)
        q3[h * 8:(h + 1) * 8, :] = jnp.where(keep, tile, 0.0)

    loads["ow"].wait()
    own_w = pltpu.make_async_copy(ow.at[:, pl.ds(pl.multiple_of(slot * 128, 128), 128)], wbuf.at[me], psem)
    own_w.start()
    loads["cg"].wait()
    loads["kc"].wait()
    loads["vc"].wait()
    pos = lax.broadcasted_iota(jnp.int32, (1, SLOTS), 1)

    def sequence(b, carry):
        used = len_ref[b]
        qb = q3[pl.ds(b, 32, stride=8), :]
        s = lax.dot_general(qb.astype(BF16), kc[b], NT, preferred_element_type=F32)
        own = jnp.sum(qb * nk[pl.ds(b, 1), :], axis=-1, keepdims=True) * 0.125
        halves = []
        for j in range(2):
            sums = cg[b, j:j + 1, :]
            latest = jnp.sum(jnp.where(pos == used - 1, sums, 0.0), axis=-1, keepdims=True)
            offsets = latest - sums + ng[j, pl.ds(b, 1), :][:, 0:1]
            scores = s[j * 16:(j + 1) * 16, :] * 0.125 + offsets
            halves.append(jnp.where(pos < used, scores, -jnp.inf))
        s = jnp.concatenate(halves, axis=0)
        top = jnp.maximum(jnp.max(s, axis=-1, keepdims=True), own)
        e = jnp.exp(s - top)
        eo = jnp.exp(own - top)
        inv = 1.0 / (jnp.sum(e, axis=-1, keepdims=True) + eo)
        mixed = jnp.dot((e * inv).astype(BF16), vc[b], preferred_element_type=F32)
        mixed = mixed + (eo * inv).astype(BF16).astype(F32) * nv[pl.ds(b, 1), :]
        o3[pl.ds(b, 32, stride=8), :] = mixed
        return carry

    lax.fori_loop(0, SEQ, sequence, 0)
    for t in range(16):
        low = o3[(2 * t) * 8:(2 * t + 1) * 8, :]
        high = o3[(2 * t + 1) * 8:(2 * t + 2) * 8, :]
        if t < 8:
            high = pltpu.roll(high, 64, 1)
        else:
            low = pltpu.roll(low, 64, 1)
        abuf[slot, :, t * 128:(t + 1) * 128] = jnp.where(lane < 64, low, high).astype(BF16)

    pl.semaphore_wait(barrier, N - 1)
    sends = []
    for k in range(1, 8):
        other = lax.rem(slot + 2 * k, 16)
        copy = remote(abuf.at[slot], abuf.at[slot], asend.at[k], arecv.at[k], group * 16 + other)
        copy.start()
        sends.append(copy)
    copy = remote(abuf.at[slot], abuf.at[slot], fwsend.at[0], arecv.at[8], partner)
    copy.start()
    sends.append(copy)

    def push(i, carry):
        peer = lax.rem(me + i, N)
        column = pl.multiple_of(lax.rem(peer, 16) * 128, 128)
        remote(ow.at[:, pl.ds(column, 128)], wbuf.at[me], wsend, wrecv, peer).start()
        return carry

    lax.fori_loop(1, N, push, 0)

    for copy in later:
        copy.wait()
    expert = me // 16
    share_row = jnp.sum(jnp.where(routes[...] == expert, shares[...], 0.0), axis=0, keepdims=True)
    for i in range(8):
        square = jnp.broadcast_to(share_row[:, i * 128:(i + 1) * 128], (128, 128))
        portion[i * 128:(i + 1) * 128, :] = square.T
    for base, extra in ((0, dg), (HPAD, du)):
        wgu[base + 480:base + HPAD, :] = jnp.zeros((HPAD - 480, D), BF16)
        wgu[base + HID:base + HID + DEN, :] = extra[...]
    wd[480:HPAD, :] = jnp.zeros((HPAD - 480, D), BF16)
    wd[HID:HID + DEN, :] = (dd[...].astype(F32) * scale[...]).astype(BF16)

    def clear(z, carry):
        acc[z] = jnp.zeros((4, 4, 2, SEQ, 2 * HPAD), F32)
        return carry

    lax.fori_loop(0, 4, clear, 0)

    for k in range(1, 8):
        source = lax.rem(slot + 16 - 2 * k, 16)
        wait_bytes(abuf.at[source], arecv.at[k])
        copy = remote(abuf.at[source], abuf.at[source], fwsend.at[k], arecv.at[8 + k], partner)
        copy.start()
        sends.append(copy)
    for k in range(8):
        wait_bytes(abuf.at[slot], arecv.at[8 + k])
    own_w.wait()
    wait_bytes(wbuf.at[pl.ds(0, N - 1)], wrecv)

    product = jnp.dot(
        abuf[...].reshape(16 * SEQ, D), wbuf[...].reshape(D, 128), preferred_element_type=F32
    )
    psend[...] = product.reshape(16, SEQ, 128)
    for k in range(1, 16):
        other = lax.rem(slot + k, 16)
        remote(psend.at[other], prec.at[slot], rsem.at[0], rsem.at[1], group * 16 + other).start()
    prec[slot] = psend[slot]
    wait_bytes(prec.at[pl.ds(0, 15)], rsem.at[1])
    projected = jnp.concatenate([prec[k] for k in range(16)], axis=-1)
    full[place[0], place[1], place[2], core] = layer_norm(
        residual_scale * tok32 + projected, gain[0:1, :], bias[0:1, :]
    )

    def cut(ref, fixed, colour, middle=(), wide=False):
        start, width, _ = COLOURS[colour]
        index = [fixed.get(axis, slice(None)) for axis in range(3)]
        columns = slice(None) if wide else pl.ds(start, width)
        return ref.at[(*index, *middle, slice(None), columns)]

    def gather_send(colour, phase, fixed):
        axis = COLOURS[colour][2][phase]
        view = cut(full, fixed, colour, (core,))
        for d in (2, 1, 3):
            remote(view, view, gsend.at[colour, phase], grecv.at[colour, phase, d - 1], peer_at(axis, d)).start()

    def gather_wait(colour, phase, d):
        order = COLOURS[colour][2]
        fixed = {a: place[a] for a in order[phase:]}
        fixed[order[phase]] = lax.rem(place[order[phase]] + 4 - d, 4)
        wait_bytes(cut(full, fixed, colour, (core,)), grecv.at[colour, phase, d - 1])
        return fixed

    def forward(colour, fixed, number):
        view = cut(full, fixed, colour, (core,))
        remote(view, view, fsend.at[colour], frecv.at[colour, number], partner).start()

    everything = dict(enumerate(place))
    for phase in range(3):
        for colour in range(3):
            gather_send(colour, phase, everything)
    for d in (1, 3, 2):
        for colour in range(3):
            fixed = gather_wait(colour, 0, d)
            gather_send(colour, 1, fixed)
            gather_send(colour, 2, fixed)
    for d in (1, 3, 2):
        for colour in range(3):
            fixed = gather_wait(colour, 1, d)
            gather_send(colour, 2, fixed)
    for colour in range(3):
        last = COLOURS[colour][2][2]
        forward(colour, {last: place[last]}, 0)

    def gate_up(i, carry):
        @pl.when(i == 1)
        def _():
            for number, d in ((1, 1), (2, 3)):
                for colour in range(3):
                    forward(colour, {COLOURS[colour][2][2]: gather_wait(colour, 2, d)[COLOURS[colour][2][2]]}, number)

        @pl.when(i == 2)
        def _():
            for colour in range(3):
                forward(colour, {COLOURS[colour][2][2]: gather_wait(colour, 2, 2)[COLOURS[colour][2][2]]}, 3)

        d = i + (i // 2) * (5 - 2 * i)
        for colour in range(3):
            start, width, order = COLOURS[colour]
            fixed = {order[2]: lax.rem(place[order[2]] + 4 - d, 4)}
            wait_bytes(cut(full, fixed, colour, (0,)), frecv.at[colour, i])
            rows = cut(full, fixed, colour, (slice(None),))[...].reshape(256, width)
            value = lax.dot_general(rows, wgu[:, start:start + width], NT, preferred_element_type=F32)
            total = cut(acc, fixed, colour, (slice(None),), wide=True)
            total[...] = total[...] + value.reshape(4, 4, 2, SEQ, 2 * HPAD)
        return carry

    lax.fori_loop(0, 4, gate_up, 0)

    column = lax.broadcasted_iota(jnp.int32, (256, HPAD), 1)

    def activate(z, carry):
        both = acc[z].reshape(256, 2 * HPAD)
        gate, up = both[:, :HPAD], both[:, HPAD:]
        weight = portion[pl.ds(pl.multiple_of(z * 256, 256), 256), :]
        weight = jnp.concatenate([weight] * 4, axis=1)
        value = gate / (1.0 + jnp.exp(-gate)) * up
        value = jnp.where(column < HID, value * weight, value)
        hid[z] = value.astype(BF16).reshape(4, 4, 2, SEQ, HPAD)
        return carry

    lax.fori_loop(0, 4, activate, 0)

    def turn(i):
        return 2 - i + (i // 2) * (7 - 2 * i)

    def scatter(i, carry):
        @pl.when(i < 4)
        def _():
            for colour in range(3):
                start, width, order = COLOURS[colour]
                fixed = {order[2]: lax.rem(place[order[2]] + turn(i), 4)}
                rows = cut(hid, fixed, colour, (slice(None),), wide=True)[...].reshape(256, HPAD)
                value = jnp.dot(rows, wd[:, start:start + width], preferred_element_type=F32)
                cut(part, fixed, colour, (slice(None),))[...] = value.astype(BF16).reshape(4, 4, 2, SEQ, width)
                remote(
                    cut(part, fixed, colour, (1 - core,)), cut(crec, fixed, colour),
                    csend.at[colour], crecv.at[colour, i], partner,
                ).start()

        @pl.when(i > 0)
        def _():
            d = turn(i - 1)
            for colour in range(3):
                order = COLOURS[colour][2]
                v3 = lax.rem(place[order[2]] + d, 4)
                fixed = {order[2]: v3}
                wait_bytes(cut(crec, fixed, colour), crecv.at[colour, i - 1])
                total = cut(part, fixed, colour, (core,))[...].astype(F32) + cut(crec, fixed, colour)[...].astype(F32)
                cut(chip, fixed, colour)[...] = total.astype(BF16)

                @pl.when(i < 4)
                def _():
                    start, width, _ = COLOURS[colour]
                    for d2 in (2, 1, 3, 0):
                        v2 = lax.rem(place[order[1]] + d2, 4)
                        remote(
                            cut(chip, {order[2]: v3, order[1]: v2}, colour),
                            r1.at[d - 1, v2, :, :, pl.ds(start, width)],
                            s1send.at[colour], s1recv.at[colour, d - 1, d2], peer_at(order[2], d),
                        ).start()

        return carry

    lax.fori_loop(0, 5, scatter, 0)

    for d2 in (2, 1, 3, 0):
        for colour in range(3):
            start, width, order = COLOURS[colour]
            columns = pl.ds(start, width)
            v2 = lax.rem(place[order[1]] + d2, 4)
            total = cut(chip, {order[2]: place[order[2]], order[1]: v2}, colour)[...].astype(F32)
            for d in (2, 1, 3):
                land = r1.at[d - 1, v2, :, :, columns]
                wait_bytes(land, s1recv.at[colour, d - 1, d2])
                total = total + land[...].astype(F32)
            t1[v2, :, :, start:start + width] = total.astype(BF16)
            if d2:
                remote(
                    t1.at[v2, :, :, columns], r2.at[d2 - 1, :, :, columns],
                    s2send.at[colour, d2 - 1], s2recv.at[colour, d2 - 1], peer_at(order[1], d2),
                ).start()
    for colour in range(3):
        start, width, order = COLOURS[colour]
        columns = pl.ds(start, width)
        total = t1[place[order[1]], :, :, start:start + width].astype(F32)
        for d in (1, 3, 2):
            land = r2.at[d - 1, :, :, columns]
            wait_bytes(land, s2recv.at[colour, d - 1])
            total = total + land[...].astype(F32)
        t2[:, :, start:start + width] = total.astype(BF16)
        for d in (2, 1, 3):
            remote(
                t2.at[lax.rem(place[order[0]] + d, 4), :, columns], r3.at[d - 1, :, columns],
                s3send.at[colour, d - 1], s3recv.at[colour, d - 1], peer_at(order[0], d),
            ).start()
    pieces = []
    for colour in range(3):
        start, width, order = COLOURS[colour]
        total = t2[place[order[0]], :, start:start + width].astype(F32)
        for d in (1, 3, 2):
            land = r3.at[d - 1, :, pl.ds(start, width)]
            wait_bytes(land, s3recv.at[colour, d - 1])
            total = total + land[...].astype(F32)
        pieces.append(total)
    base = residual_scale * full[place[0], place[1], place[2], core].astype(F32)
    out_ref[...] = layer_norm(base + jnp.concatenate(pieces, axis=-1), gain[1:2, :], bias[1:2, :])

    for copy in sends:
        copy.wait_send()
    wait_bytes(psend.at[pl.ds(0, 15)], rsem.at[0])
    wait_bytes(wbuf.at[pl.ds(0, N - 1)], wsend)
    for colour in range(3):
        start, width, order = COLOURS[colour]
        columns = pl.ds(start, width)
        wait_bytes(full.at[0, 0, pl.ds(0, 3), 0, :, columns], gsend.at[colour, 0])
        wait_bytes(full.at[0, pl.ds(0, 3), :, 0, :, columns], gsend.at[colour, 1])
        wait_bytes(full.at[pl.ds(0, 3), :, :, 0, :, columns], gsend.at[colour, 2])
        wait_bytes(full.at[:, :, :, 0, :, columns], fsend.at[colour])
        wait_bytes(crec.at[:, :, :, :, columns], csend.at[colour])
        wait_bytes(r1.at[:, :, :, :, columns], s1send.at[colour])
        for d in range(3):
            wait_bytes(r2.at[d, :, :, columns], s2send.at[colour, d])
            wait_bytes(r3.at[d, :, columns], s3send.at[colour, d])


def step(*operands):
    any_spec = pl.BlockSpec(memory_space=pl.ANY)
    dma = pltpu.SemaphoreType.DMA
    return pl.pallas_call(
        step_kernel,
        name="step",
        out_shape=jax.ShapeDtypeStruct((SEQ, D), BF16),
        in_specs=[pl.BlockSpec(memory_space=pltpu.SMEM)] + [any_spec] * 20,
        out_specs=pl.BlockSpec(memory_space=pltpu.VMEM),
        scratch_shapes=[
            pltpu.VMEM((SEQ, D), BF16),
            pltpu.VMEM((D, D), BF16),
            pltpu.VMEM((D, 128), BF16),
            pltpu.VMEM((D, 128), BF16),
            pltpu.VMEM((2, D), BF16),
            pltpu.VMEM((SEQ, SLOTS, 128), BF16),
            pltpu.VMEM((SEQ, SLOTS, 128), BF16),
            pltpu.VMEM((SEQ, 2, SLOTS), F32),
            pltpu.VMEM((16, D), BF16),
            pltpu.VMEM((2, D), F32),
            pltpu.VMEM((2, D), F32),
            pltpu.VMEM((256, 128), F32),
            pltpu.VMEM((256, 128), F32),
            pltpu.VMEM((SEQ, 128), F32),
            pltpu.VMEM((SEQ, 128), F32),
            pltpu.VMEM((2, SEQ, 128), F32),
            pltpu.VMEM((N, 16, 128), BF16),
            pltpu.VMEM((16, SEQ, D), BF16),
            pltpu.VMEM((16, SEQ, 128), F32),
            pltpu.VMEM((16, SEQ, 128), F32),
            pltpu.VMEM((4, 4, 4, 2, SEQ, D), BF16),
            pltpu.VMEM((2 * HPAD, D), BF16),
            pltpu.VMEM((HPAD, D), BF16),
            pltpu.VMEM((DEN, D), BF16),
            pltpu.VMEM((DEN, D), BF16),
            pltpu.VMEM((DEN, D), BF16),
            pltpu.VMEM((1, D), F32),
            pltpu.VMEM((2, N * SEQ), jnp.int32),
            pltpu.VMEM((2, N * SEQ), F32),
            pltpu.VMEM((N * SEQ, 128), F32),
            pltpu.VMEM((4, 4, 4, 2, SEQ, 2 * HPAD), F32),
            pltpu.VMEM((4, 4, 4, 2, SEQ, HPAD), BF16),
            pltpu.VMEM((4, 4, 4, 2, SEQ, D), BF16),
            pltpu.VMEM((4, 4, 4, SEQ, D), BF16),
            pltpu.VMEM((4, 4, 4, SEQ, D), BF16),
            pltpu.VMEM((3, 4, 4, SEQ, D), BF16),
            pltpu.VMEM((4, 4, SEQ, D), BF16),
            pltpu.VMEM((3, 4, SEQ, D), BF16),
            pltpu.VMEM((4, SEQ, D), BF16),
            pltpu.VMEM((3, SEQ, D), BF16),
            dma((16,)),
            dma((11,)),
            dma,
            dma,
            dma((8,)),
            dma((16,)),
            dma((8,)),
            dma,
            dma((2,)),
            dma((3, 3)),
            dma((3, 3, 3)),
            dma((3,)),
            dma((3, 4)),
            dma((3,)),
            dma((3, 4)),
            dma((3,)),
            dma((3, 3, 4)),
            dma((3, 3)),
            dma((3, 3)),
            dma((3, 3)),
            dma((3, 3)),
        ],
        compiler_params=pltpu.CompilerParams(
            collective_id=0, has_side_effects=True, vmem_limit_bytes=62 * 1024 * 1024
        ),
    )(*operands)


def local(
    tokens, cache_keys, cache_values, cum_gates, lengths, query_weight, key_weight, value_weight,
    forget_weight, out_weight, norm_gain, norm_bias, dense_gate_weight, dense_up_weight,
    dense_down_weight, dense_scale, expert_gate_weight, expert_up_weight, expert_down_weight,
    routes, route_weights,
):
    return step(
        lengths, tokens, query_weight, key_weight, value_weight, forget_weight.T, cache_keys, cache_values,
        jnp.transpose(cum_gates, (0, 2, 1)), out_weight, norm_gain, norm_bias, expert_gate_weight.T,
        expert_up_weight.T, expert_down_weight, dense_gate_weight.T, dense_up_weight.T, dense_down_weight,
        dense_scale.reshape(1, D), routes.T, route_weights.T,
    )


def solution(mesh):
    return jax.shard_map(
        local,
        mesh=mesh,
        in_specs=(
            P("ep", None), P("ep", None, None), P("ep", None, None), P("ep", None, None), P("ep"),
            P(), P(), P(), P(), P("ep", None), P(), P(), P(None, "ep"), P(None, "ep"), P("ep", None),
            P(), P(None, "ep"), P(None, "ep"), P("ep", None), P(), P(),
        ),
        out_specs=P("ep", None),
        check_vma=False,
    )
```

```python
import functools

import jax
import jax.numpy as jnp
from jax import lax
from jax.experimental import pallas as pl
from jax.experimental.pallas import tpu as pltpu
from jax.sharding import PartitionSpec as P

N = 128
D = 2048
SEQ = 8
SLOTS = 1024
HID = 448
DEN = 44
HPAD = 512
residual_scale = 1.4142135
norm_eps = 1e-05
MESH = pl.DeviceIdType.MESH
NT = (((1,), (1,)), ((), ()))
F32 = jnp.float32
BF16 = jnp.bfloat16

COLOURS = ((0, 768, (2, 1, 0)), (768, 768, (0, 2, 1)), (1536, 512, (1, 0, 2)))


def layer_norm(values, gain_row, shift_row):
    centre = jnp.mean(values, axis=-1, keepdims=True)
    centred = values - centre
    spread = jnp.mean(centred * centred, axis=-1, keepdims=True)
    return (centred * lax.rsqrt(spread + norm_eps) * gain_row + shift_row).astype(BF16)


def remote(src, dst, send, recv, peer):
    return pltpu.make_async_remote_copy(
        src_ref=src, dst_ref=dst, send_sem=send, recv_sem=recv, device_id=(peer,), device_id_type=MESH
    )


def wait_bytes(ref, sem):
    pltpu.make_async_copy(ref, ref, sem).wait()


def step_kernel(
    len_ref, tok_h, wq_h, wk_h, wv_h, fw_h, kc_h, vc_h, cg_h, ow_h, gain_h, bias_h,
    eg_h, eu_h, ed_h, dg_h, du_h, dd_h, scale_h, routes_h, shares_h,
    out_ref,
    tok, wq, wk, wv, fw, kc, vc, cg, ow, gain, bias,
    q3, o3, nk, nv, ng, wbuf, abuf, psend, prec,
    full, wgu, wd, dg, du, dd, scale, routes, shares, portion, acc, hid,
    part, crec, chip, r1, t1, r2, t2, r3,
    lsem, esem, wsend, wrecv, asend, arecv, psem, rsem,
    gsend, grecv, fsend, frecv, csend, crecv, s1send, s1recv, s2send, s2recv, s3send, s3recv,
):
    me = lax.axis_index("ep")
    group = me // 16
    slot = lax.rem(me, 16)
    core = lax.rem(me, 2)
    partner = me + 1 - 2 * core
    place = (me // 32, lax.rem(me // 8, 4), lax.rem(me // 2, 4))
    stride = (32, 8, 2)

    def peer_at(axis, d):
        return me + (lax.rem(place[axis] + d, 4) - place[axis]) * stride[axis]

    loads = {}

    def load(name, src, dst):
        loads[name] = pltpu.make_async_copy(src, dst, lsem.at[len(loads)])
        loads[name].start()

    load("tok", tok_h, tok)
    for k in range(8):
        load(("wq", k), wq_h.at[pl.ds(k * 256, 256)], wq.at[pl.ds(k * 256, 256)])
    load("ow", ow_h, ow)
    load("wk", wk_h, wk)
    load("wv", wv_h, wv)
    load("fw", fw_h, fw)
    load("cg", cg_h, cg)
    load("kc", kc_h, kc)
    load("vc", vc_h, vc)

    mates = [group * 16 + lax.rem(slot + k, 16) for k in range(1, 16)]
    twins = [lax.rem(me + 16 * k, N) for k in range(1, 8)]
    across = peer_at(1, 3 - 2 * lax.rem(place[1], 2))
    barrier = pltpu.get_barrier_semaphore()
    for peer in twins + mates + [across]:
        pl.semaphore_signal(barrier, inc=1, device_id=(peer,), device_id_type=MESH)
    later = []
    for src, dst in (
        (gain_h, gain), (bias_h, bias), (eg_h, wgu.at[pl.ds(0, HID)]), (eu_h, wgu.at[pl.ds(HPAD, HID)]),
        (ed_h, wd.at[pl.ds(0, HID)]), (dg_h, dg), (du_h, du), (dd_h, dd), (scale_h, scale),
        (routes_h, routes), (shares_h, shares),
    ):
        copy = pltpu.make_async_copy(src, dst, esem.at[len(later)])
        copy.start()
        later.append(copy)
    loads["tok"].wait()

    q = jnp.zeros((SEQ, D), F32)
    for k in range(8):
        loads[("wq", k)].wait()
        q = q + jnp.dot(
            tok[:, k * 256:(k + 1) * 256], wq[k * 256:(k + 1) * 256, :], preferred_element_type=F32
        )
    q = q.astype(BF16).astype(F32)
    loads["wk"].wait()
    loads["wv"].wait()
    loads["fw"].wait()
    nk[...] = jnp.dot(tok[...], wk[...], preferred_element_type=F32).astype(BF16).astype(F32)
    nv[...] = jnp.dot(tok[...], wv[...], preferred_element_type=F32).astype(BF16).astype(F32)
    tok32 = tok[...].astype(F32)
    fw32 = fw[...].astype(F32)
    for j in range(2):
        x = jnp.sum(tok32 * fw32[j:j + 1, :], axis=-1, keepdims=True)
        gate = jnp.minimum(x, 0.0) - jnp.log1p(jnp.exp(-jnp.abs(x)))
        ng[j] = jnp.broadcast_to(gate, (SEQ, 128))

    lane = lax.broadcasted_iota(jnp.int32, (SEQ, 128), 1)
    for h in range(32):
        j = h // 16
        tile = q[:, (h // 2) * 128:(h // 2 + 1) * 128]
        if h % 2 != j:
            tile = pltpu.roll(tile, 64, 1)
        keep = (lane < 64) if j == 0 else (lane >= 64)
        q3[h * 8:(h + 1) * 8, :] = jnp.where(keep, tile, 0.0)

    loads["ow"].wait()
    own_w = pltpu.make_async_copy(ow.at[:, pl.ds(pl.multiple_of(slot * 128, 128), 128)], wbuf.at[me], psem)
    own_w.start()
    pl.semaphore_wait(barrier, 23)
    for k, peer in enumerate(mates):
        column = pl.multiple_of(lax.rem(slot + k + 1, 16) * 128, 128)
        remote(ow.at[:, pl.ds(column, 128)], wbuf.at[me], wsend.at[0], wrecv.at[0], peer).start()
    loads["cg"].wait()
    loads["kc"].wait()
    loads["vc"].wait()
    pos = lax.broadcasted_iota(jnp.int32, (1, SLOTS), 1)

    def sequence(b):
        used = len_ref[b]
        qb = q3[pl.ds(b, 32, stride=8), :]
        s = lax.dot_general(qb.astype(BF16), kc[b], NT, preferred_element_type=F32)
        own = jnp.sum(qb * nk[pl.ds(b, 1), :], axis=-1, keepdims=True) * 0.125
        halves = []
        for j in range(2):
            sums = cg[b, j:j + 1, :]
            latest = jnp.sum(jnp.where(pos == used - 1, sums, 0.0), axis=-1, keepdims=True)
            offsets = latest - sums + ng[j, pl.ds(b, 1), :][:, 0:1]
            scores = s[j * 16:(j + 1) * 16, :] * 0.125 + offsets
            halves.append(jnp.where(pos < used, scores, -jnp.inf))
        s = jnp.concatenate(halves, axis=0)
        top = jnp.maximum(jnp.max(s, axis=-1, keepdims=True), own)
        e = jnp.exp(s - top)
        eo = jnp.exp(own - top)
        inv = 1.0 / (jnp.sum(e, axis=-1, keepdims=True) + eo)
        mixed = jnp.dot((e * inv).astype(BF16), vc[b], preferred_element_type=F32)
        mixed = mixed + (eo * inv).astype(BF16).astype(F32) * nv[pl.ds(b, 1), :]
        o3[pl.ds(b, 32, stride=8), :] = mixed

    def sequences(i, carry):
        for b in range(4):
            sequence(4 * i + b)
        return carry

    lax.fori_loop(0, SEQ // 4, sequences, 0)
    for t in range(16):
        low = o3[(2 * t) * 8:(2 * t + 1) * 8, :]
        high = o3[(2 * t + 1) * 8:(2 * t + 2) * 8, :]
        if t < 8:
            high = pltpu.roll(high, 64, 1)
        else:
            low = pltpu.roll(low, 64, 1)
        abuf[slot, :, t * 128:(t + 1) * 128] = jnp.where(lane < 64, low, high).astype(BF16)

    for k in range(1, 8):
        other = lax.rem(slot + 2 * k, 16)
        remote(abuf.at[slot], abuf.at[slot], asend.at[0], arecv.at[k], group * 16 + other).start()
    remote(abuf.at[slot], abuf.at[slot], asend.at[1], arecv.at[0], partner).start()
    own_w.wait()
    wait_bytes(wbuf.at[pl.ds(0, 15)], wrecv.at[0])
    rows_here = pl.ds(group * 16, 16)
    for peer in twins:
        remote(wbuf.at[rows_here], wbuf.at[rows_here], wsend.at[1], wrecv.at[1], peer).start()

    for copy in later:
        copy.wait()
    expert = me // 16
    share_row = jnp.sum(jnp.where(routes[...] == expert, shares[...], 0.0), axis=0, keepdims=True)
    for i in range(8):
        square = jnp.broadcast_to(share_row[:, i * 128:(i + 1) * 128], (128, 128))
        portion[i * 128:(i + 1) * 128, :] = square.T
    for base, extra in ((0, dg), (HPAD, du)):
        wgu[base + 480:base + HPAD, :] = jnp.zeros((HPAD - 480, D), BF16)
        wgu[base + HID:base + HID + DEN, :] = extra[...]
    wd[480:HPAD, :] = jnp.zeros((HPAD - 480, D), BF16)
    wd[HID:HID + DEN, :] = (dd[...].astype(F32) * scale[...]).astype(BF16)

    def clear(z, carry):
        acc[z] = jnp.zeros((4, 4, 2, SEQ, 2 * HPAD), F32)
        return carry

    lax.fori_loop(0, 4, clear, 0)

    for k in range(1, 8):
        source = lax.rem(slot + 16 - 2 * k, 16)
        wait_bytes(abuf.at[source], arecv.at[k])
        remote(abuf.at[source], abuf.at[source], asend.at[1], arecv.at[0], partner).start()
    wait_bytes(abuf.at[pl.ds(0, 8)], arecv.at[0])
    wait_bytes(wbuf.at[pl.ds(0, N - 16)], wrecv.at[1])

    product = jnp.dot(
        abuf[...].reshape(16 * SEQ, D), wbuf[...].reshape(D, 128), preferred_element_type=F32
    )
    psend[...] = product.reshape(16, SEQ, 128)
    for k in range(1, 16):
        other = lax.rem(slot + k, 16)
        remote(psend.at[other], prec.at[slot], rsem.at[0], rsem.at[1], group * 16 + other).start()
    prec[slot] = psend[slot]
    wait_bytes(prec.at[pl.ds(0, 15)], rsem.at[1])
    projected = jnp.concatenate([prec[k] for k in range(16)], axis=-1)
    full[place[0], place[1], place[2], core] = layer_norm(
        residual_scale * tok32 + projected, gain[0:1, :], bias[0:1, :]
    )

    def cut(ref, fixed, colour, middle=(), wide=False):
        start, width, _ = COLOURS[colour]
        index = [fixed.get(axis, slice(None)) for axis in range(3)]
        columns = slice(None) if wide else pl.ds(start, width)
        return ref.at[(*index, *middle, slice(None), columns)]

    def gather_send(colour, phase, fixed, number=0):
        axis = COLOURS[colour][2][phase]
        view = cut(full, fixed, colour, (core,))
        for d in (1, 3, 2):
            remote(
                view, view, gsend.at[phase], grecv.at[phase if phase < 2 else 2 + number, d - 1], peer_at(axis, d)
            ).start()

    def gather_wait(phase, d, number=0):
        wait_bytes(
            full.at[0, 0, pl.ds(0, 4 if phase else 1), 0], grecv.at[phase if phase < 2 else 2 + number, d - 1]
        )
        pieces = []
        for _, _, order in COLOURS:
            fixed = {a: place[a] for a in order[phase:]}
            fixed[order[phase]] = lax.rem(place[order[phase]] + 4 - d, 4)
            if phase == 2:
                fixed[order[1]] = lax.rem(place[order[1]] + 4 - number, 4)
            pieces.append(fixed)
        return pieces

    def forward(colour, fixed, number):
        view = cut(full, fixed, colour, (core,))
        remote(view, view, fsend.at[0], frecv.at[number], partner).start()

    def gather_last(number):
        for d in (1, 3, 2):
            for colour, fixed in enumerate(gather_wait(2, d, number)):
                forward(colour, fixed, number)

    def gate_up(colour, number):
        start, width, order = COLOURS[colour]
        fixed = {order[1]: lax.rem(place[order[1]] + 4 - number, 4)}
        if colour == 0:
            wait_bytes(full.at[:, :, 0, 0], frecv.at[number])
        rows = cut(full, fixed, colour, (slice(None),))[...].reshape(256, width)
        total = cut(acc, fixed, colour, (slice(None),), wide=True)
        value = total[...].reshape(256, 2 * HPAD) + lax.dot_general(
            rows, wgu[:, start:start + width], NT, preferred_element_type=F32
        )
        total[...] = value.reshape(4, 4, 2, SEQ, 2 * HPAD)

    everything = dict(enumerate(place))
    for phase in range(3):
        for colour in range(3):
            gather_send(colour, phase, everything)
    for d in (1, 3, 2):
        for colour, fixed in enumerate(gather_wait(0, d)):
            gather_send(colour, 1, fixed)
            gather_send(colour, 2, fixed)
    for colour in range(3):
        order = COLOURS[colour][2]
        forward(colour, {order[1]: place[order[1]], order[2]: place[order[2]]}, 0)
    for d in (1, 3, 2):
        for colour, fixed in enumerate(gather_wait(1, d)):
            gather_send(colour, 2, fixed, d)
            forward(colour, fixed, d)
    gather_last(0)
    for colour in range(3):
        gate_up(colour, 0)
    gather_last(1)
    gather_last(3)
    for colour in range(3):
        gate_up(colour, 1)
    gate_up(0, 3)
    gather_last(2)
    for colour in range(1, 3):
        gate_up(colour, 3)
    for colour in range(3):
        gate_up(colour, 2)

    column = lax.broadcasted_iota(jnp.int32, (256, HPAD), 1)

    def activate(z, carry):
        both = acc[z].reshape(256, 2 * HPAD)
        gate, up = both[:, :HPAD], both[:, HPAD:]
        weight = portion[pl.ds(pl.multiple_of(z * 256, 256), 256), :]
        weight = jnp.concatenate([weight] * 4, axis=1)
        value = gate / (1.0 + jnp.exp(-gate)) * up
        value = jnp.where(column < HID, value * weight, value)
        hid[z] = value.astype(BF16).reshape(4, 4, 2, SEQ, HPAD)
        return carry

    lax.fori_loop(0, 4, activate, 0)

    def turn(i):
        return 2 - i + (i // 2) * (7 - 2 * i)

    def product_of(i, colour):
        start, width, order = COLOURS[colour]
        fixed = {order[1]: lax.rem(place[order[1]] + turn(i), 4)}
        rows = cut(hid, fixed, colour, (slice(None),), wide=True)[...].reshape(256, HPAD)
        value = jnp.dot(rows, wd[:, start:start + width], preferred_element_type=F32)
        cut(part, fixed, colour, (slice(None),))[...] = value.astype(BF16).reshape(4, 4, 2, SEQ, width)
        remote(
            cut(part, fixed, colour, (1 - core,)), cut(crec, fixed, colour),
            csend.at[0], crecv.at[colour, i], partner,
        ).start()

    def join(i, colour):
        start, width, order = COLOURS[colour]
        v2 = lax.rem(place[order[1]] + turn(i), 4)
        fixed = {order[1]: v2}
        wait_bytes(cut(crec, fixed, colour), crecv.at[colour, i])
        total = cut(part, fixed, colour, (core,))[...].astype(F32) + cut(crec, fixed, colour)[...].astype(F32)
        cut(chip, fixed, colour)[...] = total.astype(BF16)
        for d in (2, 1, 3):
            remote(
                cut(chip, {order[2]: lax.rem(place[order[2]] + d, 4), order[1]: v2}, colour),
                r1.at[d - 1, v2, :, :, pl.ds(start, width)],
                s1send.at[0], s1recv.at[colour, turn(i)], peer_at(order[2], d),
            ).start()

    def scatter(i, carry):
        for colour in range(3):
            @pl.when(i < 4)
            def _(colour=colour):
                product_of(i, colour)

            @pl.when(i > 0)
            def _(colour=colour):
                join(i - 1, colour)

        return carry

    lax.fori_loop(0, 5, scatter, 0)
    wait_bytes(abuf.at[pl.ds(0, 7)], asend.at[0])
    wait_bytes(abuf.at[pl.ds(0, 8)], asend.at[1])
    wait_bytes(psend.at[pl.ds(0, 15)], rsem.at[0])
    wait_bytes(wbuf.at[pl.ds(0, 15)], wsend.at[0])
    wait_bytes(wbuf.at[pl.ds(0, N - 16)], wsend.at[1])
    wait_bytes(full.at[0, 0, pl.ds(0, 3), 0], gsend.at[0])
    wait_bytes(full.at[0, pl.ds(0, 3), :, 0], gsend.at[1])
    wait_bytes(full.at[pl.ds(0, 3), :, :, 0], gsend.at[2])
    wait_bytes(full.at[:, :, :, 0], fsend.at[0])
    wait_bytes(crec, csend.at[0])
    for d2 in (2, 1, 3, 0):
        for colour in range(3):
            start, width, order = COLOURS[colour]
            columns = pl.ds(start, width)
            v2 = lax.rem(place[order[1]] + d2, 4)
            total = cut(chip, {order[2]: place[order[2]], order[1]: v2}, colour)[...].astype(F32)
            wait_bytes(r1.at[:, v2, :, :, columns], s1recv.at[colour, d2])
            for d in range(3):
                total = total + r1[d, v2, :, :, start:start + width].astype(F32)
            t1[v2, :, :, start:start + width] = total.astype(BF16)
            if d2:
                remote(
                    t1.at[v2, :, :, columns], r2.at[d2 - 1, :, :, columns],
                    s2send.at[0], s2recv.at[colour], peer_at(order[1], d2),
                ).start()
    for colour in range(3):
        start, width, order = COLOURS[colour]
        columns = pl.ds(start, width)
        total = t1[place[order[1]], :, :, start:start + width].astype(F32)
        wait_bytes(r2.at[:, :, :, columns], s2recv.at[colour])
        for d in range(3):
            total = total + r2[d, :, :, start:start + width].astype(F32)
        t2[:, :, start:start + width] = total.astype(BF16)
        for d in (2, 1, 3):
            remote(
                t2.at[lax.rem(place[order[0]] + d, 4), :, columns], r3.at[d - 1, :, columns],
                s3send.at[0], s3recv.at[colour], peer_at(order[0], d),
            ).start()
    wait_bytes(r1, s1send.at[0])
    wait_bytes(r2, s2send.at[0])
    pieces = []
    for colour in range(3):
        start, width, order = COLOURS[colour]
        total = t2[place[order[0]], :, start:start + width].astype(F32)
        wait_bytes(r3.at[:, :, pl.ds(start, width)], s3recv.at[colour])
        for d in range(3):
            total = total + r3[d, :, start:start + width].astype(F32)
        pieces.append(total)
    base = residual_scale * full[place[0], place[1], place[2], core].astype(F32)
    out_ref[...] = layer_norm(base + jnp.concatenate(pieces, axis=-1), gain[1:2, :], bias[1:2, :])

    wait_bytes(r3, s3send.at[0])


def step(*operands):
    any_spec = pl.BlockSpec(memory_space=pl.ANY)
    dma = pltpu.SemaphoreType.DMA
    return pl.pallas_call(
        step_kernel,
        name="step",
        out_shape=jax.ShapeDtypeStruct((SEQ, D), BF16),
        in_specs=[pl.BlockSpec(memory_space=pltpu.SMEM)] + [any_spec] * 20,
        out_specs=pl.BlockSpec(memory_space=pltpu.VMEM),
        scratch_shapes=[
            pltpu.VMEM((SEQ, D), BF16),
            pltpu.VMEM((D, D), BF16),
            pltpu.VMEM((D, 128), BF16),
            pltpu.VMEM((D, 128), BF16),
            pltpu.VMEM((2, D), BF16),
            pltpu.VMEM((SEQ, SLOTS, 128), BF16),
            pltpu.VMEM((SEQ, SLOTS, 128), BF16),
            pltpu.VMEM((SEQ, 2, SLOTS), F32),
            pltpu.VMEM((16, D), BF16),
            pltpu.VMEM((2, D), F32),
            pltpu.VMEM((2, D), F32),
            pltpu.VMEM((256, 128), F32),
            pltpu.VMEM((256, 128), F32),
            pltpu.VMEM((SEQ, 128), F32),
            pltpu.VMEM((SEQ, 128), F32),
            pltpu.VMEM((2, SEQ, 128), F32),
            pltpu.VMEM((N, 16, 128), BF16),
            pltpu.VMEM((16, SEQ, D), BF16),
            pltpu.VMEM((16, SEQ, 128), F32),
            pltpu.VMEM((16, SEQ, 128), F32),
            pltpu.VMEM((4, 4, 4, 2, SEQ, D), BF16),
            pltpu.VMEM((2 * HPAD, D), BF16),
            pltpu.VMEM((HPAD, D), BF16),
            pltpu.VMEM((DEN, D), BF16),
            pltpu.VMEM((DEN, D), BF16),
            pltpu.VMEM((DEN, D), BF16),
            pltpu.VMEM((1, D), F32),
            pltpu.VMEM((2, N * SEQ), jnp.int32),
            pltpu.VMEM((2, N * SEQ), F32),
            pltpu.VMEM((N * SEQ, 128), F32),
            pltpu.VMEM((4, 4, 4, 2, SEQ, 2 * HPAD), F32),
            pltpu.VMEM((4, 4, 4, 2, SEQ, HPAD), BF16),
            pltpu.VMEM((4, 4, 4, 2, SEQ, D), BF16),
            pltpu.VMEM((4, 4, 4, SEQ, D), BF16),
            pltpu.VMEM((4, 4, 4, SEQ, D), BF16),
            pltpu.VMEM((3, 4, 4, SEQ, D), BF16),
            pltpu.VMEM((4, 4, SEQ, D), BF16),
            pltpu.VMEM((3, 4, SEQ, D), BF16),
            pltpu.VMEM((4, SEQ, D), BF16),
            pltpu.VMEM((3, SEQ, D), BF16),
            dma((16,)),
            dma((11,)),
            dma((2,)),
            dma((2,)),
            dma((2,)),
            dma((8,)),
            dma,
            dma((2,)),
            dma((3,)),
            dma((6, 3)),
            dma((1,)),
            dma((4,)),
            dma((1,)),
            dma((3, 4)),
            dma((1,)),
            dma((3, 4)),
            dma((1,)),
            dma((3,)),
            dma((1,)),
            dma((3,)),
        ],
        compiler_params=pltpu.CompilerParams(
            collective_id=0, has_side_effects=True, vmem_limit_bytes=62 * 1024 * 1024
        ),
    )(*operands)


def local(
    tokens, cache_keys, cache_values, cum_gates, lengths, query_weight, key_weight, value_weight,
    forget_weight, out_weight, norm_gain, norm_bias, dense_gate_weight, dense_up_weight,
    dense_down_weight, dense_scale, expert_gate_weight, expert_up_weight, expert_down_weight,
    routes, route_weights,
):
    return step(
        lengths, tokens, query_weight, key_weight, value_weight, forget_weight.T, cache_keys, cache_values,
        jnp.transpose(cum_gates, (0, 2, 1)), out_weight, norm_gain, norm_bias, expert_gate_weight.T,
        expert_up_weight.T, expert_down_weight, dense_gate_weight.T, dense_up_weight.T, dense_down_weight,
        dense_scale.reshape(1, D), routes.T, route_weights.T,
    )


def solution(mesh):
    return jax.shard_map(
        local,
        mesh=mesh,
        in_specs=(
            P("ep", None), P("ep", None, None), P("ep", None, None), P("ep", None, None), P("ep"),
            P(), P(), P(), P(), P("ep", None), P(), P(), P(None, "ep"), P(None, "ep"), P("ep", None),
            P(), P(None, "ep"), P(None, "ep"), P("ep", None), P(), P(),
        ),
        out_specs=P("ep", None),
        check_vma=False,
    )
```

```python
import functools

import jax
import jax.numpy as jnp
from jax import lax
from jax.experimental import pallas as pl
from jax.experimental.pallas import tpu as pltpu
from jax.sharding import PartitionSpec as P

N = 128
D = 2048
SEQ = 8
SLOTS = 1024
HID = 448
DEN = 44
HPAD = 512
residual_scale = 1.4142135
norm_eps = 1e-05
MESH = pl.DeviceIdType.MESH
NT = (((1,), (1,)), ((), ()))
F32 = jnp.float32
BF16 = jnp.bfloat16

COLOURS = ((0, 768, (2, 1, 0)), (768, 768, (0, 2, 1)), (1536, 512, (1, 0, 2)))


def layer_norm(values, gain_row, shift_row):
    centre = jnp.mean(values, axis=-1, keepdims=True)
    centred = values - centre
    spread = jnp.mean(centred * centred, axis=-1, keepdims=True)
    return (centred * lax.rsqrt(spread + norm_eps) * gain_row + shift_row).astype(BF16)


def remote(src, dst, send, recv, peer):
    return pltpu.make_async_remote_copy(
        src_ref=src, dst_ref=dst, send_sem=send, recv_sem=recv, device_id=(peer,), device_id_type=MESH
    )


def wait_bytes(ref, sem):
    pltpu.make_async_copy(ref, ref, sem).wait()


def step_kernel(
    len_ref, tok_h, wq_h, wk_h, wv_h, fw_h, kc_h, vc_h, cg_h, ow_h, gain_h, bias_h,
    eg_h, eu_h, ed_h, dg_h, du_h, dd_h, scale_h, routes_h, shares_h,
    out_ref,
    tok, wq, wk, wv, fw, kc, vc, cg, ow, gain, bias,
    q3, o3, nk, nv, ng, wpair, wbuf, abuf, psend, prec,
    full, wgu, wd, dg, du, dd, scale, routes, shares, portion, acc, hid,
    part, crec, chip, r1, t1, r2,
    lsem, esem, wsend, wrecv, asend, arecv, psem, rsem,
    gsend, grecv, fsend, frecv, csend, crecv, s1send, s1recv, s2send, s2recv,
):
    me = lax.axis_index("ep")
    group = me // 16
    slot = lax.rem(me, 16)
    core = lax.rem(me, 2)
    partner = me + 1 - 2 * core
    place = (me // 32, lax.rem(me // 8, 4), lax.rem(me // 2, 4))
    stride = (32, 8, 2)

    def peer_at(*moves):
        return me + sum((lax.rem(place[axis] + d, 4) - place[axis]) * stride[axis] for axis, d in moves)

    loads = {}

    def load(name, src, dst):
        loads[name] = pltpu.make_async_copy(src, dst, lsem.at[len(loads)])
        loads[name].start()

    load("tok", tok_h, tok)
    for k in range(8):
        load(("wq", k), wq_h.at[pl.ds(k * 256, 256)], wq.at[pl.ds(k * 256, 256)])
    load("ow", ow_h, ow)
    load("wk", wk_h, wk)
    load("wv", wv_h, wv)
    load("fw", fw_h, fw)
    load("cg", cg_h, cg)
    load("kc", kc_h, kc)
    load("vc", vc_h, vc)

    barrier = pltpu.get_barrier_semaphore()
    for peer in [lax.rem(me + 2 * i, N) for i in range(1, N // 2)] + [
        group * 16 + lax.rem(slot + k, 16) for k in range(1, 16, 2)
    ]:
        pl.semaphore_signal(barrier, inc=1, device_id=(peer,), device_id_type=MESH)
    loads["tok"].wait()

    q = jnp.zeros((SEQ, D), F32)
    for k in range(8):
        loads[("wq", k)].wait()
        q = q + jnp.dot(
            tok[:, k * 256:(k + 1) * 256], wq[k * 256:(k + 1) * 256, :], preferred_element_type=F32
        )
    later = []
    for src, dst in (
        (gain_h, gain), (bias_h, bias), (eg_h, wgu.at[pl.ds(0, HID)]), (eu_h, wgu.at[pl.ds(HPAD, HID)]),
        (ed_h, wd.at[pl.ds(0, HID)]), (dg_h, dg), (du_h, du), (dd_h, dd), (scale_h, scale),
        (routes_h, routes), (shares_h, shares),
    ):
        copy = pltpu.make_async_copy(src, dst, esem.at[len(later)])
        copy.start()
        later.append(copy)
    q = q.astype(BF16).astype(F32)
    loads["wk"].wait()
    loads["wv"].wait()
    loads["fw"].wait()
    nk[...] = jnp.dot(tok[...], wk[...], preferred_element_type=F32).astype(BF16).astype(F32)
    nv[...] = jnp.dot(tok[...], wv[...], preferred_element_type=F32).astype(BF16).astype(F32)
    tok32 = tok[...].astype(F32)
    fw32 = fw[...].astype(F32)
    for j in range(2):
        x = jnp.sum(tok32 * fw32[j:j + 1, :], axis=-1, keepdims=True)
        gate = jnp.minimum(x, 0.0) - jnp.log1p(jnp.exp(-jnp.abs(x)))
        ng[j] = jnp.broadcast_to(gate, (SEQ, 128))

    lane = lax.broadcasted_iota(jnp.int32, (SEQ, 128), 1)
    for h in range(32):
        j = h // 16
        tile = q[:, (h // 2) * 128:(h // 2 + 1) * 128]
        if h % 2 != j:
            tile = pltpu.roll(tile, 64, 1)
        keep = (lane < 64) if j == 0 else (lane >= 64)
        q3[h * 8:(h + 1) * 8, :] = jnp.where(keep, tile, 0.0)

    loads["ow"].wait()
    own_columns = pl.ds(pl.multiple_of(slot // 2 * 256, 256), 256)
    own_w = pltpu.make_async_copy(ow.at[:, own_columns], wpair.at[me // 2], psem)
    own_w.start()
    loads["cg"].wait()
    loads["kc"].wait()
    loads["vc"].wait()
    pos = lax.broadcasted_iota(jnp.int32, (1, SLOTS), 1)

    def sequence(b):
        used = len_ref[b]
        qb = q3[pl.ds(b, 32, stride=8), :]
        s = lax.dot_general(qb.astype(BF16), kc[b], NT, preferred_element_type=F32)
        own = jnp.sum(qb * nk[pl.ds(b, 1), :], axis=-1, keepdims=True) * 0.125
        halves = []
        for j in range(2):
            sums = cg[b, j:j + 1, :]
            latest = jnp.sum(jnp.where(pos == used - 1, sums, 0.0), axis=-1, keepdims=True)
            offsets = latest - sums + ng[j, pl.ds(b, 1), :][:, 0:1]
            scores = s[j * 16:(j + 1) * 16, :] * 0.125 + offsets
            halves.append(jnp.where(pos < used, scores, -jnp.inf))
        s = jnp.concatenate(halves, axis=0)
        top = jnp.maximum(jnp.max(s, axis=-1, keepdims=True), own)
        e = jnp.exp(s - top)
        eo = jnp.exp(own - top)
        inv = 1.0 / (jnp.sum(e, axis=-1, keepdims=True) + eo)
        mixed = jnp.dot((e * inv).astype(BF16), vc[b], preferred_element_type=F32)
        mixed = mixed + (eo * inv).astype(BF16).astype(F32) * nv[pl.ds(b, 1), :]
        o3[pl.ds(b, 32, stride=8), :] = mixed

    def push_columns():
        pl.semaphore_wait(barrier, N // 2 + 7)
        for i in range(1, N // 2):
            peer = lax.rem(me + 2 * i, N)
            columns = pl.ds(pl.multiple_of(lax.rem(peer, 16) // 2 * 256, 256), 256)
            remote(ow.at[:, columns], wpair.at[me // 2], wsend.at[0], wrecv.at[0], peer).start()

    def sequences(i, carry):
        @pl.when(i == 1)
        def _():
            push_columns()

        for b in range(2):
            sequence(2 * i + b)
        return carry

    lax.fori_loop(0, SEQ // 2, sequences, 0)
    for t in range(16):
        low = o3[(2 * t) * 8:(2 * t + 1) * 8, :]
        high = o3[(2 * t + 1) * 8:(2 * t + 2) * 8, :]
        if t < 8:
            high = pltpu.roll(high, 64, 1)
        else:
            low = pltpu.roll(low, 64, 1)
        abuf[slot, :, t * 128:(t + 1) * 128] = jnp.where(lane < 64, low, high).astype(BF16)

    for k in range(1, 8):
        other = lax.rem(slot + 2 * k, 16)
        remote(abuf.at[slot], abuf.at[slot], asend.at[0], arecv.at[k], group * 16 + other).start()
    remote(abuf.at[slot], abuf.at[slot], asend.at[1], arecv.at[0], partner).start()
    for copy in later:
        copy.wait()
    expert = me // 16
    share_row = jnp.sum(jnp.where(routes[...] == expert, shares[...], 0.0), axis=0, keepdims=True)
    for i in range(8):
        square = jnp.broadcast_to(share_row[:, i * 128:(i + 1) * 128], (128, 128))
        portion[i * 128:(i + 1) * 128, :] = square.T
    for base, extra in ((0, dg), (HPAD, du)):
        wgu[base + 480:base + HPAD, :] = jnp.zeros((HPAD - 480, D), BF16)
        wgu[base + HID:base + HID + DEN, :] = extra[...]
    wd[480:HPAD, :] = jnp.zeros((HPAD - 480, D), BF16)
    wd[HID:HID + DEN, :] = (dd[...].astype(F32) * scale[...]).astype(BF16)

    def clear(z, carry):
        acc[z] = jnp.zeros((4, 4, 2, SEQ, 2 * HPAD), F32)
        return carry

    lax.fori_loop(0, 4, clear, 0)

    for k in range(1, 8):
        source = lax.rem(slot + 16 - 2 * k, 16)
        wait_bytes(abuf.at[source], arecv.at[k])
        remote(abuf.at[source], abuf.at[source], asend.at[1], arecv.at[0], partner).start()
    own_w.wait()
    wait_bytes(wpair.at[pl.ds(0, N // 2 - 1)], wrecv.at[0])
    half = pl.ds(pl.multiple_of((1 - core) * 128, 128), 128)
    remote(wpair.at[:, :, half], wbuf.at[:, core], wsend.at[1], wrecv.at[1], partner).start()
    wbuf[:, core] = jnp.where(core == 0, wpair[:, :, :128], wpair[:, :, 128:])
    wait_bytes(abuf.at[pl.ds(0, 8)], arecv.at[0])
    wait_bytes(wbuf.at[:, 0], wrecv.at[1])

    product = jnp.dot(
        abuf[...].reshape(16 * SEQ, D), wbuf[...].reshape(D, 128), preferred_element_type=F32
    )
    psend[...] = product.reshape(16, SEQ, 128)
    for k in range(1, 16):
        other = lax.rem(slot + k, 16)
        remote(psend.at[other], prec.at[slot], rsem.at[0], rsem.at[1], group * 16 + other).start()
    prec[slot] = psend[slot]
    wait_bytes(prec.at[pl.ds(0, 15)], rsem.at[1])
    projected = jnp.concatenate([prec[k] for k in range(16)], axis=-1)
    full[place[0], place[1], place[2], core] = layer_norm(
        residual_scale * tok32 + projected, gain[0:1, :], bias[0:1, :]
    )

    def cut(ref, fixed, colour, middle=(), wide=False):
        start, width, _ = COLOURS[colour]
        index = [fixed.get(axis, slice(None)) for axis in range(3)]
        columns = slice(None) if wide else pl.ds(start, width)
        return ref.at[(*index, *middle, slice(None), columns)]

    everything = dict(enumerate(place))

    def gather_plane(number):
        for d1 in (0, 1, 3, 2):
            for colour, (_, _, order) in enumerate(COLOURS):
                if d1 or number:
                    view = cut(full, everything, colour, (core,))
                    where = grecv.at[1, number - 1] if number else grecv.at[0, d1 - 1]
                    remote(view, view, gsend.at[min(number, 1)], where, peer_at((order[0], d1), (order[1], number))).start()

    def gather_send(colour, fixed, number=0):
        view = cut(full, fixed, colour, (core,))
        for d in (1, 3, 2):
            remote(view, view, gsend.at[2], grecv.at[2 + number, d - 1], peer_at((COLOURS[colour][2][2], d))).start()

    def gather_wait(phase, d, number=0):
        wait_bytes(
            full.at[0, 0, pl.ds(0, 4 if phase else 1), 0], grecv.at[phase if phase < 2 else 2 + number, d - 1]
        )
        pieces = []
        for _, _, order in COLOURS:
            fixed = {a: place[a] for a in order[phase:]}
            fixed[order[phase]] = lax.rem(place[order[phase]] + 4 - d, 4)
            if phase == 2:
                fixed[order[1]] = lax.rem(place[order[1]] + 4 - number, 4)
            pieces.append(fixed)
        return pieces

    def forward(colour, fixed, number):
        view = cut(full, fixed, colour, (core,))
        remote(view, view, fsend.at[0], frecv.at[number], partner).start()

    def gather_last(number):
        for d in (1, 3, 2):
            for colour, fixed in enumerate(gather_wait(2, d, number)):
                forward(colour, fixed, number)

    def gate_up(colour, *numbers):
        start, width, order = COLOURS[colour]
        rows, totals = [], []
        for number in numbers:
            fixed = {order[1]: lax.rem(place[order[1]] + 4 - number, 4)}
            if colour == 0:
                wait_bytes(full.at[:, :, 0, 0], frecv.at[number])
            rows.append(cut(full, fixed, colour, (slice(None),))[...].reshape(256, width))
            totals.append(cut(acc, fixed, colour, (slice(None),), wide=True))
        value = lax.dot_general(
            jnp.concatenate(rows, axis=0), wgu[:, start:start + width], NT, preferred_element_type=F32
        )
        for i, total in enumerate(totals):
            total[...] = total[...] + value[i * 256:(i + 1) * 256].reshape(4, 4, 2, SEQ, 2 * HPAD)

    for number in (0, 1, 3, 2):
        gather_plane(number)
    for colour in range(3):
        gather_send(colour, everything)
    for d in (1, 3, 2):
        for colour, fixed in enumerate(gather_wait(0, d)):
            gather_send(colour, fixed)
    for colour in range(3):
        order = COLOURS[colour][2]
        forward(colour, {order[1]: place[order[1]], order[2]: place[order[2]]}, 0)
    for d in (1, 3, 2):
        for colour, fixed in enumerate(gather_wait(1, d)):
            gather_send(colour, fixed, d)
            forward(colour, fixed, d)
    gather_last(0)
    gate_up(0, 0)
    gather_last(1)
    gate_up(1, 0)
    gather_last(3)
    gate_up(2, 0)
    gate_up(0, 1, 3)
    gather_last(2)
    for colour in range(1, 3):
        gate_up(colour, 1, 3)
    for colour in range(3):
        gate_up(colour, 2)

    column = lax.broadcasted_iota(jnp.int32, (256, HPAD), 1)

    def activate(z, carry):
        both = acc[z].reshape(256, 2 * HPAD)
        gate, up = both[:, :HPAD], both[:, HPAD:]
        weight = portion[pl.ds(pl.multiple_of(z * 256, 256), 256), :]
        weight = jnp.concatenate([weight] * 4, axis=1)
        value = gate / (1.0 + jnp.exp(-gate)) * up
        value = jnp.where(column < HID, value * weight, value)
        hid[z] = value.astype(BF16).reshape(4, 4, 2, SEQ, HPAD)
        return carry

    lax.fori_loop(0, 4, activate, 0)

    def turn(i):
        return 2 - i + (i // 2) * (7 - 2 * i)

    def product_of(i, colour):
        start, width, order = COLOURS[colour]
        fixed = {order[1]: lax.rem(place[order[1]] + turn(i), 4)}
        rows = cut(hid, fixed, colour, (slice(None),), wide=True)[...].reshape(256, HPAD)
        value = jnp.dot(rows, wd[:, start:start + width], preferred_element_type=F32)
        cut(part, fixed, colour, (slice(None),))[...] = value.astype(BF16).reshape(4, 4, 2, SEQ, width)
        remote(
            cut(part, fixed, colour, (1 - core,)), cut(crec, fixed, colour),
            csend.at[0], crecv.at[colour, i], partner,
        ).start()

    def join(i, colour):
        start, width, order = COLOURS[colour]
        v2 = lax.rem(place[order[1]] + turn(i), 4)
        fixed = {order[1]: v2}
        wait_bytes(cut(crec, fixed, colour), crecv.at[colour, i])
        total = cut(part, fixed, colour, (core,))[...].astype(F32) + cut(crec, fixed, colour)[...].astype(F32)
        cut(chip, fixed, colour)[...] = total.astype(BF16)
        for d in (2, 1, 3):
            remote(
                cut(chip, {order[2]: lax.rem(place[order[2]] + d, 4), order[1]: v2}, colour),
                r1.at[d - 1, v2, :, :, pl.ds(start, width)],
                s1send.at[0], s1recv.at[colour, turn(i)], peer_at((order[2], d)),
            ).start()

    def scatter(i, carry):
        for colour in range(3):
            @pl.when(i < 4)
            def _(colour=colour):
                product_of(i, colour)

            @pl.when(i > 0)
            def _(colour=colour):
                join(i - 1, colour)

        return carry

    lax.fori_loop(0, 5, scatter, 0)
    wait_bytes(abuf.at[pl.ds(0, 7)], asend.at[0])
    wait_bytes(abuf.at[pl.ds(0, 8)], asend.at[1])
    wait_bytes(psend.at[pl.ds(0, 15)], rsem.at[0])
    wait_bytes(wpair.at[pl.ds(0, N // 2 - 1)], wsend.at[0])
    wait_bytes(wbuf.at[:, 0], wsend.at[1])
    wait_bytes(full.at[0, 0, pl.ds(0, 3), 0], gsend.at[0])
    wait_bytes(full.at[0, pl.ds(0, 3), :, 0], gsend.at[1])
    wait_bytes(full.at[pl.ds(0, 3), :, :, 0], gsend.at[2])
    wait_bytes(full.at[:, :, :, 0], fsend.at[0])
    wait_bytes(crec, csend.at[0])
    for d2 in (2, 1, 3, 0):
        for colour in range(3):
            start, width, order = COLOURS[colour]
            columns = pl.ds(start, width)
            v2 = lax.rem(place[order[1]] + d2, 4)
            total = cut(chip, {order[2]: place[order[2]], order[1]: v2}, colour)[...].astype(F32)
            wait_bytes(r1.at[:, v2, :, :, columns], s1recv.at[colour, d2])
            for d in range(3):
                total = total + r1[d, v2, :, :, start:start + width].astype(F32)
            t1[v2, :, :, start:start + width] = total.astype(BF16)
            for d1 in (2, 1, 3, 0):
                if d1 or d2:
                    remote(
                        t1.at[v2, lax.rem(place[order[0]] + d1, 4), :, columns], r2.at[4 * d2 + d1, :, columns],
                        s2send.at[0], s2recv.at[colour], peer_at((order[0], d1), (order[1], d2)),
                    ).start()
    wait_bytes(r1, s1send.at[0])
    pieces = []
    for colour in range(3):
        start, width, order = COLOURS[colour]
        total = t1[place[order[1]], place[order[0]], :, start:start + width].astype(F32)
        wait_bytes(r2.at[pl.ds(1, 15), :, pl.ds(start, width)], s2recv.at[colour])
        for d in range(1, 16):
            total = total + r2[d, :, start:start + width].astype(F32)
        pieces.append(total)
    base = residual_scale * full[place[0], place[1], place[2], core].astype(F32)
    out_ref[...] = layer_norm(base + jnp.concatenate(pieces, axis=-1), gain[1:2, :], bias[1:2, :])

    wait_bytes(r2.at[pl.ds(1, 15)], s2send.at[0])


def step(*operands):
    any_spec = pl.BlockSpec(memory_space=pl.ANY)
    dma = pltpu.SemaphoreType.DMA
    return pl.pallas_call(
        step_kernel,
        name="step",
        out_shape=jax.ShapeDtypeStruct((SEQ, D), BF16),
        in_specs=[pl.BlockSpec(memory_space=pltpu.SMEM)] + [any_spec] * 20,
        out_specs=pl.BlockSpec(memory_space=pltpu.VMEM),
        scratch_shapes=[
            pltpu.VMEM((SEQ, D), BF16),
            pltpu.VMEM((D, D), BF16),
            pltpu.VMEM((D, 128), BF16),
            pltpu.VMEM((D, 128), BF16),
            pltpu.VMEM((2, D), BF16),
            pltpu.VMEM((SEQ, SLOTS, 128), BF16),
            pltpu.VMEM((SEQ, SLOTS, 128), BF16),
            pltpu.VMEM((SEQ, 2, SLOTS), F32),
            pltpu.VMEM((16, D), BF16),
            pltpu.VMEM((2, D), F32),
            pltpu.VMEM((2, D), F32),
            pltpu.VMEM((256, 128), F32),
            pltpu.VMEM((256, 128), F32),
            pltpu.VMEM((SEQ, 128), F32),
            pltpu.VMEM((SEQ, 128), F32),
            pltpu.VMEM((2, SEQ, 128), F32),
            pltpu.VMEM((N // 2, 16, 256), BF16),
            pltpu.VMEM((N // 2, 2, 16, 128), BF16),
            pltpu.VMEM((16, SEQ, D), BF16),
            pltpu.VMEM((16, SEQ, 128), F32),
            pltpu.VMEM((16, SEQ, 128), F32),
            pltpu.VMEM((4, 4, 4, 2, SEQ, D), BF16),
            pltpu.VMEM((2 * HPAD, D), BF16),
            pltpu.VMEM((HPAD, D), BF16),
            pltpu.VMEM((DEN, D), BF16),
            pltpu.VMEM((DEN, D), BF16),
            pltpu.VMEM((DEN, D), BF16),
            pltpu.VMEM((1, D), F32),
            pltpu.VMEM((2, N * SEQ), jnp.int32),
            pltpu.VMEM((2, N * SEQ), F32),
            pltpu.VMEM((N * SEQ, 128), F32),
            pltpu.VMEM((4, 4, 4, 2, SEQ, 2 * HPAD), F32),
            pltpu.VMEM((4, 4, 4, 2, SEQ, HPAD), BF16),
            pltpu.VMEM((4, 4, 4, 2, SEQ, D), BF16),
            pltpu.VMEM((4, 4, 4, SEQ, D), BF16),
            pltpu.VMEM((4, 4, 4, SEQ, D), BF16),
            pltpu.VMEM((3, 4, 4, SEQ, D), BF16),
            pltpu.VMEM((4, 4, SEQ, D), BF16),
            pltpu.VMEM((16, SEQ, D), BF16),
            dma((16,)),
            dma((11,)),
            dma((2,)),
            dma((2,)),
            dma((2,)),
            dma((8,)),
            dma,
            dma((2,)),
            dma((3,)),
            dma((6, 3)),
            dma((1,)),
            dma((4,)),
            dma((1,)),
            dma((3, 4)),
            dma((1,)),
            dma((3, 4)),
            dma((1,)),
            dma((3,)),
        ],
        compiler_params=pltpu.CompilerParams(
            collective_id=0, has_side_effects=True, vmem_limit_bytes=62 * 1024 * 1024
        ),
    )(*operands)


def local(
    tokens, cache_keys, cache_values, cum_gates, lengths, query_weight, key_weight, value_weight,
    forget_weight, out_weight, norm_gain, norm_bias, dense_gate_weight, dense_up_weight,
    dense_down_weight, dense_scale, expert_gate_weight, expert_up_weight, expert_down_weight,
    routes, route_weights,
):
    return step(
        lengths, tokens, query_weight, key_weight, value_weight, forget_weight.T, cache_keys, cache_values,
        jnp.transpose(cum_gates, (0, 2, 1)), out_weight, norm_gain, norm_bias, expert_gate_weight.T,
        expert_up_weight.T, expert_down_weight, dense_gate_weight.T, dense_up_weight.T, dense_down_weight,
        dense_scale.reshape(1, D), routes.T, route_weights.T,
    )


def solution(mesh):
    return jax.shard_map(
        local,
        mesh=mesh,
        in_specs=(
            P("ep", None), P("ep", None, None), P("ep", None, None), P("ep", None, None), P("ep"),
            P(), P(), P(), P(), P("ep", None), P(), P(), P(None, "ep"), P(None, "ep"), P("ep", None),
            P(), P(None, "ep"), P(None, "ep"), P("ep", None), P(), P(),
        ),
        out_specs=P("ep", None),
        check_vma=False,
    )
```

```python
import functools

import jax
import jax.numpy as jnp
from jax import lax
from jax.experimental import pallas as pl
from jax.experimental.pallas import tpu as pltpu
from jax.sharding import PartitionSpec as P

N = 128
D = 2048
SEQ = 8
SLOTS = 1024
HID = 448
DEN = 44
HPAD = 512
residual_scale = 1.4142135
norm_eps = 1e-05
MESH = pl.DeviceIdType.MESH
NT = (((1,), (1,)), ((), ()))
F32 = jnp.float32
BF16 = jnp.bfloat16

COLOURS = ((0, 768, (2, 1, 0)), (768, 768, (0, 2, 1)), (1536, 512, (1, 0, 2)))


CHIPS = sorted(range(1, N // 2), key=lambda i: -sum(min(i // s % 4, 4 - i // s % 4) for s in (16, 4, 1)))
MATES = ((0, 1), (0, 3), (1, 0), (0, 2), (1, 1), (1, 3), (1, 2))


def layer_norm(values, gain_row, shift_row):
    centre = jnp.mean(values, axis=-1, keepdims=True)
    centred = values - centre
    spread = jnp.mean(centred * centred, axis=-1, keepdims=True)
    return (centred * lax.rsqrt(spread + norm_eps) * gain_row + shift_row).astype(BF16)


def remote(src, dst, send, recv, peer):
    return pltpu.make_async_remote_copy(
        src_ref=src, dst_ref=dst, send_sem=send, recv_sem=recv, device_id=(peer,), device_id_type=MESH
    )


def wait_bytes(ref, sem):
    pltpu.make_async_copy(ref, ref, sem).wait()


def step_kernel(
    len_ref, tok_h, wq_h, wk_h, wv_h, fw_h, kc_h, vc_h, cg_h, ow_h, gain_h, bias_h,
    eg_h, eu_h, ed_h, dg_h, du_h, dd_h, scale_h, routes_h, shares_h,
    out_ref,
    tok, wq, wk, wv, fw, kc, vc, cg, ow, gain, bias,
    q3, o3, nk, nv, ng, wpair, wbuf, abuf, psend, prec,
    full, wgu, wd, dg, du, dd, scale, routes, shares, portion, acc, hid,
    part, crec, chip, r1, t1, r2,
    lsem, esem, wsend, wrecv, asend, arecv, psem, rsem,
    gsend, grecv, fsend, frecv, csend, crecv, s1send, s1recv, s2send, s2recv,
):
    me = lax.axis_index("ep")
    group = me // 16
    slot = lax.rem(me, 16)
    core = lax.rem(me, 2)
    partner = me + 1 - 2 * core
    place = (me // 32, lax.rem(me // 8, 4), lax.rem(me // 2, 4))
    stride = (32, 8, 2)

    def peer_at(*moves):
        return me + sum((lax.rem(place[axis] + d, 4) - place[axis]) * stride[axis] for axis, d in moves)

    loads = {}

    def load(name, src, dst):
        loads[name] = pltpu.make_async_copy(src, dst, lsem.at[len(loads)])
        loads[name].start()

    load("tok", tok_h, tok)
    for k in range(8):
        load(("wq", k), wq_h.at[pl.ds(k * 256, 256)], wq.at[pl.ds(k * 256, 256)])
    load("ow", ow_h, ow)
    load("wk", wk_h, wk)
    load("wv", wv_h, wv)
    load("fw", fw_h, fw)
    load("cg", cg_h, cg)
    load("kc", kc_h, kc)
    load("vc", vc_h, vc)

    barrier = pltpu.get_barrier_semaphore()
    for peer in [lax.rem(me + 2 * i, N) for i in CHIPS] + [
        group * 16 + lax.rem(slot + k, 16) for k in range(1, 16, 2)
    ]:
        pl.semaphore_signal(barrier, inc=1, device_id=(peer,), device_id_type=MESH)
    loads["tok"].wait()

    q = jnp.zeros((SEQ, D), F32)
    for k in range(8):
        loads[("wq", k)].wait()
        q = q + jnp.dot(
            tok[:, k * 256:(k + 1) * 256], wq[k * 256:(k + 1) * 256, :], preferred_element_type=F32
        )
    later = []
    for src, dst in (
        (gain_h, gain), (bias_h, bias), (eg_h, wgu.at[pl.ds(0, HID)]), (eu_h, wgu.at[pl.ds(HPAD, HID)]),
        (ed_h, wd.at[pl.ds(0, HID)]), (dg_h, dg), (du_h, du), (dd_h, dd), (scale_h, scale),
        (routes_h, routes), (shares_h, shares),
    ):
        copy = pltpu.make_async_copy(src, dst, esem.at[len(later)])
        copy.start()
        later.append(copy)
    q = q.astype(BF16).astype(F32)
    loads["wk"].wait()
    loads["wv"].wait()
    loads["fw"].wait()
    nk[...] = jnp.dot(tok[...], wk[...], preferred_element_type=F32).astype(BF16).astype(F32)
    nv[...] = jnp.dot(tok[...], wv[...], preferred_element_type=F32).astype(BF16).astype(F32)
    tok32 = tok[...].astype(F32)
    fw32 = fw[...].astype(F32)
    for j in range(2):
        x = jnp.sum(tok32 * fw32[j:j + 1, :], axis=-1, keepdims=True)
        gate = jnp.minimum(x, 0.0) - jnp.log1p(jnp.exp(-jnp.abs(x)))
        ng[j] = jnp.broadcast_to(gate, (SEQ, 128))

    lane = lax.broadcasted_iota(jnp.int32, (SEQ, 128), 1)
    for h in range(32):
        j = h // 16
        tile = q[:, (h // 2) * 128:(h // 2 + 1) * 128]
        if h % 2 != j:
            tile = pltpu.roll(tile, 64, 1)
        keep = (lane < 64) if j == 0 else (lane >= 64)
        q3[h * 8:(h + 1) * 8, :] = jnp.where(keep, tile, 0.0)

    loads["ow"].wait()
    own_columns = pl.ds(pl.multiple_of(slot // 2 * 256, 256), 256)
    own_w = pltpu.make_async_copy(ow.at[:, own_columns], wpair.at[me // 2], psem)
    own_w.start()
    def push_columns():
        pl.semaphore_wait(barrier, N // 2 + 7)
        for i in CHIPS:
            peer = lax.rem(me + 2 * i, N)
            columns = pl.ds(pl.multiple_of(lax.rem(peer, 16) // 2 * 256, 256), 256)
            remote(ow.at[:, columns], wpair.at[me // 2], wsend.at[0], wrecv.at[0], peer).start()

    push_columns()
    loads["cg"].wait()
    loads["kc"].wait()
    loads["vc"].wait()
    pos = lax.broadcasted_iota(jnp.int32, (1, SLOTS), 1)

    def sequence(b):
        used = len_ref[b]
        qb = q3[pl.ds(b, 32, stride=8), :]
        s = lax.dot_general(qb.astype(BF16), kc[b], NT, preferred_element_type=F32)
        own = jnp.sum(qb * nk[pl.ds(b, 1), :], axis=-1, keepdims=True) * 0.125
        halves = []
        for j in range(2):
            sums = cg[b, j:j + 1, :]
            latest = jnp.sum(jnp.where(pos == used - 1, sums, 0.0), axis=-1, keepdims=True)
            offsets = latest - sums + ng[j, pl.ds(b, 1), :][:, 0:1]
            scores = s[j * 16:(j + 1) * 16, :] * 0.125 + offsets
            halves.append(jnp.where(pos < used, scores, -jnp.inf))
        s = jnp.concatenate(halves, axis=0)
        top = jnp.maximum(jnp.max(s, axis=-1, keepdims=True), own)
        e = jnp.exp(s - top)
        eo = jnp.exp(own - top)
        inv = 1.0 / (jnp.sum(e, axis=-1, keepdims=True) + eo)
        mixed = jnp.dot((e * inv).astype(BF16), vc[b], preferred_element_type=F32)
        mixed = mixed + (eo * inv).astype(BF16).astype(F32) * nv[pl.ds(b, 1), :]
        o3[pl.ds(b, 32, stride=8), :] = mixed

    def sequences(i, carry):
        for b in range(2):
            sequence(2 * i + b)
        return carry

    lax.fori_loop(0, SEQ // 2, sequences, 0)
    for t in range(16):
        low = o3[(2 * t) * 8:(2 * t + 1) * 8, :]
        high = o3[(2 * t + 1) * 8:(2 * t + 2) * 8, :]
        if t < 8:
            high = pltpu.roll(high, 64, 1)
        else:
            low = pltpu.roll(low, 64, 1)
        abuf[slot, :, t * 128:(t + 1) * 128] = jnp.where(lane < 64, low, high).astype(BF16)

    def mate(dy, dx):
        return lax.rem(slot // 8 + dy, 2) * 8 + lax.rem(place[2] + dx, 4) * 2 + core

    for k, (dy, dx) in enumerate(MATES):
        remote(
            abuf.at[slot], abuf.at[slot], asend.at[0], arecv.at[k + 1], group * 16 + mate(dy, dx)
        ).start()
    remote(abuf.at[slot], abuf.at[slot], asend.at[1], arecv.at[0], partner).start()
    for copy in later:
        copy.wait()
    expert = me // 16
    share_row = jnp.sum(jnp.where(routes[...] == expert, shares[...], 0.0), axis=0, keepdims=True)
    for i in range(8):
        square = jnp.broadcast_to(share_row[:, i * 128:(i + 1) * 128], (128, 128))
        portion[i * 128:(i + 1) * 128, :] = square.T
    for base, extra in ((0, dg), (HPAD, du)):
        wgu[base + 480:base + HPAD, :] = jnp.zeros((HPAD - 480, D), BF16)
        wgu[base + HID:base + HID + DEN, :] = extra[...]
    wd[480:HPAD, :] = jnp.zeros((HPAD - 480, D), BF16)
    wd[HID:HID + DEN, :] = (dd[...].astype(F32) * scale[...]).astype(BF16)

    def clear(z, carry):
        acc[z] = jnp.zeros((4, 4, 2, SEQ, 2 * HPAD), F32)
        return carry

    lax.fori_loop(0, 4, clear, 0)

    for k, (dy, dx) in enumerate(MATES):
        source = mate(dy, 4 - dx)
        wait_bytes(abuf.at[source], arecv.at[k + 1])
        remote(abuf.at[source], abuf.at[source], asend.at[1], arecv.at[0], partner).start()
    own_w.wait()
    wait_bytes(wpair.at[pl.ds(0, N // 2 - 1)], wrecv.at[0])
    half = pl.ds(pl.multiple_of((1 - core) * 128, 128), 128)
    remote(wpair.at[:, :, half], wbuf.at[:, core], wsend.at[1], wrecv.at[1], partner).start()
    wbuf[:, core] = jnp.where(core == 0, wpair[:, :, :128], wpair[:, :, 128:])
    wait_bytes(abuf.at[pl.ds(0, 8)], arecv.at[0])
    wait_bytes(wbuf.at[:, 0], wrecv.at[1])

    product = jnp.dot(
        abuf[...].reshape(16 * SEQ, D), wbuf[...].reshape(D, 128), preferred_element_type=F32
    )
    psend[...] = product.reshape(16, SEQ, 128)
    for k in range(1, 16):
        other = lax.rem(slot + k, 16)
        remote(psend.at[other], prec.at[slot], rsem.at[0], rsem.at[1], group * 16 + other).start()
    prec[slot] = psend[slot]
    wait_bytes(prec.at[pl.ds(0, 15)], rsem.at[1])
    projected = jnp.concatenate([prec[k] for k in range(16)], axis=-1)
    full[place[0], place[1], place[2], core] = layer_norm(
        residual_scale * tok32 + projected, gain[0:1, :], bias[0:1, :]
    )

    def cut(ref, fixed, colour, middle=(), wide=False):
        start, width, _ = COLOURS[colour]
        index = [fixed.get(axis, slice(None)) for axis in range(3)]
        columns = slice(None) if wide else pl.ds(start, width)
        return ref.at[(*index, *middle, slice(None), columns)]

    everything = dict(enumerate(place))

    def gather_plane(number):
        for d1 in (0, 1, 3, 2):
            for colour, (_, _, order) in enumerate(COLOURS):
                if d1 or number:
                    view = cut(full, everything, colour, (core,))
                    where = grecv.at[1, number - 1] if number else grecv.at[0, d1 - 1]
                    remote(view, view, gsend.at[min(number, 1)], where, peer_at((order[0], d1), (order[1], number))).start()

    def gather_send(colour, fixed, number=0):
        view = cut(full, fixed, colour, (core,))
        for d in (1, 3, 2):
            remote(view, view, gsend.at[2], grecv.at[2 + number, d - 1], peer_at((COLOURS[colour][2][2], d))).start()

    def gather_wait(phase, d, number=0):
        wait_bytes(
            full.at[0, 0, pl.ds(0, 4 if phase else 1), 0], grecv.at[phase if phase < 2 else 2 + number, d - 1]
        )
        pieces = []
        for _, _, order in COLOURS:
            fixed = {a: place[a] for a in order[phase:]}
            fixed[order[phase]] = lax.rem(place[order[phase]] + 4 - d, 4)
            if phase == 2:
                fixed[order[1]] = lax.rem(place[order[1]] + 4 - number, 4)
            pieces.append(fixed)
        return pieces

    def forward(colour, fixed, number):
        view = cut(full, fixed, colour, (core,))
        remote(view, view, fsend.at[0], frecv.at[number], partner).start()

    def gather_last(number):
        for d in (1, 3, 2):
            for colour, fixed in enumerate(gather_wait(2, d, number)):
                forward(colour, fixed, number)

    def gate_up(colour, *numbers):
        start, width, order = COLOURS[colour]
        rows, totals = [], []
        for number in numbers:
            fixed = {order[1]: lax.rem(place[order[1]] + 4 - number, 4)}
            if colour == 0:
                wait_bytes(full.at[:, :, 0, 0], frecv.at[number])
            rows.append(cut(full, fixed, colour, (slice(None),))[...].reshape(256, width))
            totals.append(cut(acc, fixed, colour, (slice(None),), wide=True))
        value = lax.dot_general(
            jnp.concatenate(rows, axis=0), wgu[:, start:start + width], NT, preferred_element_type=F32
        )
        for i, total in enumerate(totals):
            total[...] = total[...] + value[i * 256:(i + 1) * 256].reshape(4, 4, 2, SEQ, 2 * HPAD)

    for number in (0, 1, 3, 2):
        gather_plane(number)
    for colour in range(3):
        gather_send(colour, everything)
    for d in (1, 3, 2):
        for colour, fixed in enumerate(gather_wait(0, d)):
            gather_send(colour, fixed)
    for colour in range(3):
        order = COLOURS[colour][2]
        forward(colour, {order[1]: place[order[1]], order[2]: place[order[2]]}, 0)
    for d in (1, 3, 2):
        for colour, fixed in enumerate(gather_wait(1, d)):
            gather_send(colour, fixed, d)
            forward(colour, fixed, d)
    gather_last(0)
    gate_up(0, 0)
    gather_last(1)
    gate_up(1, 0)
    gather_last(3)
    gate_up(2, 0)
    gate_up(0, 1, 3)
    gather_last(2)
    for colour in range(1, 3):
        gate_up(colour, 1, 3)
    for colour in range(3):
        gate_up(colour, 2)

    column = lax.broadcasted_iota(jnp.int32, (256, HPAD), 1)

    def activate(z, carry):
        both = acc[z].reshape(256, 2 * HPAD)
        gate, up = both[:, :HPAD], both[:, HPAD:]
        weight = portion[pl.ds(pl.multiple_of(z * 256, 256), 256), :]
        weight = jnp.concatenate([weight] * 4, axis=1)
        value = gate / (1.0 + jnp.exp(-gate)) * up
        value = jnp.where(column < HID, value * weight, value)
        hid[z] = value.astype(BF16).reshape(4, 4, 2, SEQ, HPAD)
        return carry

    lax.fori_loop(0, 4, activate, 0)

    def turn(i):
        return 2 - i + (i // 2) * (7 - 2 * i)

    def product_of(i, colour):
        start, width, order = COLOURS[colour]
        fixed = {order[1]: lax.rem(place[order[1]] + turn(i), 4)}
        rows = cut(hid, fixed, colour, (slice(None),), wide=True)[...].reshape(256, HPAD)
        value = jnp.dot(rows, wd[:, start:start + width], preferred_element_type=F32)
        cut(part, fixed, colour, (slice(None),))[...] = value.astype(BF16).reshape(4, 4, 2, SEQ, width)
        remote(
            cut(part, fixed, colour, (1 - core,)), cut(crec, fixed, colour),
            csend.at[0], crecv.at[colour, i], partner,
        ).start()

    def join(i, colour):
        start, width, order = COLOURS[colour]
        v2 = lax.rem(place[order[1]] + turn(i), 4)
        fixed = {order[1]: v2}
        wait_bytes(cut(crec, fixed, colour), crecv.at[colour, i])
        total = cut(part, fixed, colour, (core,))[...].astype(F32) + cut(crec, fixed, colour)[...].astype(F32)
        cut(chip, fixed, colour)[...] = total.astype(BF16)
        for d in (2, 1, 3):
            remote(
                cut(chip, {order[2]: lax.rem(place[order[2]] + d, 4), order[1]: v2}, colour),
                r1.at[d - 1, v2, :, :, pl.ds(start, width)],
                s1send.at[0], s1recv.at[colour, turn(i)], peer_at((order[2], d)),
            ).start()

    def scatter(i, carry):
        for colour in range(3):
            @pl.when(i < 4)
            def _(colour=colour):
                product_of(i, colour)

            @pl.when(i > 0)
            def _(colour=colour):
                join(i - 1, colour)

        return carry

    lax.fori_loop(0, 5, scatter, 0)
    wait_bytes(abuf.at[pl.ds(0, 7)], asend.at[0])
    wait_bytes(abuf.at[pl.ds(0, 8)], asend.at[1])
    wait_bytes(psend.at[pl.ds(0, 15)], rsem.at[0])
    wait_bytes(wpair.at[pl.ds(0, N // 2 - 1)], wsend.at[0])
    wait_bytes(wbuf.at[:, 0], wsend.at[1])
    wait_bytes(full.at[0, 0, pl.ds(0, 3), 0], gsend.at[0])
    wait_bytes(full.at[0, pl.ds(0, 3), :, 0], gsend.at[1])
    wait_bytes(full.at[pl.ds(0, 3), :, :, 0], gsend.at[2])
    wait_bytes(full.at[:, :, :, 0], fsend.at[0])
    wait_bytes(crec, csend.at[0])
    for d2 in (2, 1, 3, 0):
        for colour in range(3):
            start, width, order = COLOURS[colour]
            columns = pl.ds(start, width)
            v2 = lax.rem(place[order[1]] + d2, 4)
            total = cut(chip, {order[2]: place[order[2]], order[1]: v2}, colour)[...].astype(F32)
            wait_bytes(r1.at[:, v2, :, :, columns], s1recv.at[colour, d2])
            for d in range(3):
                total = total + r1[d, v2, :, :, start:start + width].astype(F32)
            t1[v2, :, :, start:start + width] = total.astype(BF16)
            for d1 in (2, 1, 3, 0):
                if d1 or d2:
                    remote(
                        t1.at[v2, lax.rem(place[order[0]] + d1, 4), :, columns], r2.at[4 * d2 + d1, :, columns],
                        s2send.at[0], s2recv.at[colour], peer_at((order[0], d1), (order[1], d2)),
                    ).start()
    wait_bytes(r1, s1send.at[0])
    pieces = []
    for colour in range(3):
        start, width, order = COLOURS[colour]
        total = t1[place[order[1]], place[order[0]], :, start:start + width].astype(F32)
        wait_bytes(r2.at[pl.ds(1, 15), :, pl.ds(start, width)], s2recv.at[colour])
        for d in range(1, 16):
            total = total + r2[d, :, start:start + width].astype(F32)
        pieces.append(total)
    base = residual_scale * full[place[0], place[1], place[2], core].astype(F32)
    out_ref[...] = layer_norm(base + jnp.concatenate(pieces, axis=-1), gain[1:2, :], bias[1:2, :])

    wait_bytes(r2.at[pl.ds(1, 15)], s2send.at[0])


def step(*operands):
    any_spec = pl.BlockSpec(memory_space=pl.ANY)
    dma = pltpu.SemaphoreType.DMA
    return pl.pallas_call(
        step_kernel,
        name="step",
        out_shape=jax.ShapeDtypeStruct((SEQ, D), BF16),
        in_specs=[pl.BlockSpec(memory_space=pltpu.SMEM)] + [any_spec] * 20,
        out_specs=pl.BlockSpec(memory_space=pltpu.VMEM),
        scratch_shapes=[
            pltpu.VMEM((SEQ, D), BF16),
            pltpu.VMEM((D, D), BF16),
            pltpu.VMEM((D, 128), BF16),
            pltpu.VMEM((D, 128), BF16),
            pltpu.VMEM((2, D), BF16),
            pltpu.VMEM((SEQ, SLOTS, 128), BF16),
            pltpu.VMEM((SEQ, SLOTS, 128), BF16),
            pltpu.VMEM((SEQ, 2, SLOTS), F32),
            pltpu.VMEM((16, D), BF16),
            pltpu.VMEM((2, D), F32),
            pltpu.VMEM((2, D), F32),
            pltpu.VMEM((256, 128), F32),
            pltpu.VMEM((256, 128), F32),
            pltpu.VMEM((SEQ, 128), F32),
            pltpu.VMEM((SEQ, 128), F32),
            pltpu.VMEM((2, SEQ, 128), F32),
            pltpu.VMEM((N // 2, 16, 256), BF16),
            pltpu.VMEM((N // 2, 2, 16, 128), BF16),
            pltpu.VMEM((16, SEQ, D), BF16),
            pltpu.VMEM((16, SEQ, 128), F32),
            pltpu.VMEM((16, SEQ, 128), F32),
            pltpu.VMEM((4, 4, 4, 2, SEQ, D), BF16),
            pltpu.VMEM((2 * HPAD, D), BF16),
            pltpu.VMEM((HPAD, D), BF16),
            pltpu.VMEM((DEN, D), BF16),
            pltpu.VMEM((DEN, D), BF16),
            pltpu.VMEM((DEN, D), BF16),
            pltpu.VMEM((1, D), F32),
            pltpu.VMEM((2, N * SEQ), jnp.int32),
            pltpu.VMEM((2, N * SEQ), F32),
            pltpu.VMEM((N * SEQ, 128), F32),
            pltpu.VMEM((4, 4, 4, 2, SEQ, 2 * HPAD), F32),
            pltpu.VMEM((4, 4, 4, 2, SEQ, HPAD), BF16),
            pltpu.VMEM((4, 4, 4, 2, SEQ, D), BF16),
            pltpu.VMEM((4, 4, 4, SEQ, D), BF16),
            pltpu.VMEM((4, 4, 4, SEQ, D), BF16),
            pltpu.VMEM((3, 4, 4, SEQ, D), BF16),
            pltpu.VMEM((4, 4, SEQ, D), BF16),
            pltpu.VMEM((16, SEQ, D), BF16),
            dma((16,)),
            dma((11,)),
            dma((2,)),
            dma((2,)),
            dma((2,)),
            dma((8,)),
            dma,
            dma((2,)),
            dma((3,)),
            dma((6, 3)),
            dma((1,)),
            dma((4,)),
            dma((1,)),
            dma((3, 4)),
            dma((1,)),
            dma((3, 4)),
            dma((1,)),
            dma((3,)),
        ],
        compiler_params=pltpu.CompilerParams(
            collective_id=0, has_side_effects=True, vmem_limit_bytes=62 * 1024 * 1024
        ),
    )(*operands)


def local(
    tokens, cache_keys, cache_values, cum_gates, lengths, query_weight, key_weight, value_weight,
    forget_weight, out_weight, norm_gain, norm_bias, dense_gate_weight, dense_up_weight,
    dense_down_weight, dense_scale, expert_gate_weight, expert_up_weight, expert_down_weight,
    routes, route_weights,
):
    return step(
        lengths, tokens, query_weight, key_weight, value_weight, forget_weight.T, cache_keys, cache_values,
        jnp.transpose(cum_gates, (0, 2, 1)), out_weight, norm_gain, norm_bias, expert_gate_weight.T,
        expert_up_weight.T, expert_down_weight, dense_gate_weight.T, dense_up_weight.T, dense_down_weight,
        dense_scale.reshape(1, D), routes.T, route_weights.T,
    )


def solution(mesh):
    return jax.shard_map(
        local,
        mesh=mesh,
        in_specs=(
            P("ep", None), P("ep", None, None), P("ep", None, None), P("ep", None, None), P("ep"),
            P(), P(), P(), P(), P("ep", None), P(), P(), P(None, "ep"), P(None, "ep"), P("ep", None),
            P(), P(None, "ep"), P(None, "ep"), P("ep", None), P(), P(),
        ),
        out_specs=P("ep", None),
        check_vma=False,
    )
```
